32 devices in a mesh: sp: 16 (over z, y, x), tp: 2 (over core).
Axes of the slice: x: 2, y: 2, z: 4, core: 2. Of those that a mesh axis runs over, the one named last changes fastest.
Arguments:
- latent: bfloat16 [4096, 2048], P(('sp', 'tp')), may hold values from -6 to 6
- cond: float32 [2048], replicated, may hold values from -6 to 6
- ctx_mod: float32 [2048], replicated, may hold values from -6 to 6
- context: bfloat16 [512, 2048], P(('sp', 'tp')), may hold values from -6 to 6
- shift_w: float32 [2048, 2048], P('sp', 'tp'), may hold values from -0.125 to 0.125
- scale_w: float32 [2048, 2048], P('sp', 'tp'), may hold values from -0.125 to 0.125
- gate_w: float32 [2048, 2048], P('sp', 'tp'), may hold values from -0.125 to 0.125
- norm_gain: float32 [2048], replicated, may hold values from 0.1 to 1.9
- w_qn: bfloat16 [2048, 2048], P(None, 'tp'), may hold values from -0.125 to 0.125
- w_qr: bfloat16 [2048, 1024], P(None, 'tp'), may hold values from -0.13258252 to 0.13258252
- w_kv_down: bfloat16 [2048, 512], replicated, may hold values from -0.125 to 0.125
- w_rope_key: bfloat16 [2048, 64], replicated, may hold values from -0.13258252 to 0.13258252
- kv_gain: float32 [512], replicated, may hold values from 0.1 to 1.9
- w_key_up: bfloat16 [512, 2048], P(None, 'tp'), may hold values from -0.66015625 to 0.66015625
- w_value_up: bfloat16 [512, 2048], P(None, 'tp'), may hold values from -0.25 to 0.25
- ctx_bias: float32 [16], P('tp'), may hold values from 2 to 3.5
- w_out: bfloat16 [2048, 2048], P('tp'), may hold values from -0.52734375 to 0.52734375
Outputs:
- mixed: bfloat16 [4096, 2048], P(('sp', 'tp'))
The draws below stay inside these ranges and needn't reach their ends.
All inputs are finite; a program needn't handle non-finite values.
Results may differ from the reference program's by a relative error of at most 0.018.
Values may be sent and summed in bfloat16 or wider, within the bound.
A program may use at most 128 MiB of HBM per device.

```python
import jax
import jax.numpy as jnp
from jax import lax

D = 2048
HEADS = 16
NOPE = 128
ROPE = 64
VDIM = 128
KV_RANK = 512
GRID_W = 128
CTX = 512
SEQ = 4096
HEADS_DEV = 8
N_TP = 2


def weight_base(key, shape):
    return jax.random.normal(key, shape, jnp.float32) * D ** (-0.5)


def draw_latent(key, part):
    tokens = jax.random.normal(jax.random.fold_in(key, 1), (SEQ, D), jnp.float32)
    return jnp.clip(tokens, -6.0, 6.0).astype(jnp.bfloat16)


def draw_w_qr(key, part):
    matrix = weight_base(jax.random.fold_in(key, 5), (D, HEADS * ROPE))
    bound = 6.0 * D ** (-0.5)
    return jnp.clip(matrix, -bound, bound).astype(jnp.bfloat16)


def draw_w_rope_key(key, part):
    matrix = weight_base(jax.random.fold_in(key, 6), (D, ROPE))
    bound = 6.0 * D ** (-0.5)
    return jnp.clip(matrix, -bound, bound).astype(jnp.bfloat16)


def steps_of(own_key, shape, cuts, smallest, largest):
    loudness = 1.0
    for position, shards_of in cuts:
        steps = jax.random.uniform(jax.random.fold_in(jax.random.fold_in(own_key, 6), position), (shards_of,), jnp.float32, smallest / len(cuts), largest / len(cuts))
        loudness = loudness * jnp.repeat(jnp.exp(steps), shape[position] // shards_of).reshape((-1,) + (1,) * (len(shape) - 1 - position))
    return loudness


def bell_draw(key, extent, deviation, most, split=(), kind=jnp.bfloat16):
    loudness = steps_of(key, extent, split, -0.22, 0.18) if split else 1.0
    array = jax.random.normal(key, extent, jnp.float32) * deviation * loudness
    return jnp.minimum(jnp.maximum(array, -most), most).astype(kind)


def setup_inputs(seed: int = 0) -> dict:
    seeds = jax.random.split(jax.random.key(seed), 18)
    return {
        "latent": draw_latent(jax.random.fold_in(seeds[17], 71), 0),
        "cond": bell_draw(seeds[1], (D,), 1.0, 6.0, (), jnp.float32),
        "ctx_mod": bell_draw(seeds[2], (D,), 1.0, 6.0, (), jnp.float32),
        "context": bell_draw(seeds[3], (CTX, D), 1.0, 6.0, ((0, 32),)),
        "shift_w": bell_draw(seeds[4], (D, D), D ** -0.5, 0.125, ((0, 16), (1, 2)), jnp.float32),
        "scale_w": bell_draw(seeds[5], (D, D), D ** -0.5, 0.125, ((0, 16), (1, 2)), jnp.float32),
        "gate_w": bell_draw(seeds[6], (D, D), D ** -0.5, 0.125, ((0, 16), (1, 2)), jnp.float32),
        "norm_gain": jnp.clip(1.0 + 0.18 * jax.random.normal(seeds[7], (D,), jnp.float32), 0.1, 1.9),
        "w_qn": bell_draw(seeds[8], (D, HEADS * NOPE), D ** -0.5, 0.125, ((1, 2),)),
        "w_qr": draw_w_qr(jax.random.fold_in(seeds[17], 71), 0),
        "w_kv_down": bell_draw(seeds[10], (D, KV_RANK), D ** -0.5, 0.125),
        "w_rope_key": draw_w_rope_key(jax.random.fold_in(seeds[17], 71), 0),
        "kv_gain": jnp.clip(1.0 + 0.18 * jax.random.normal(seeds[12], (KV_RANK,), jnp.float32), 0.1, 1.9),
        "w_key_up": bell_draw(seeds[13], (KV_RANK, HEADS * NOPE), (2.5 * KV_RANK ** -0.5), 0.66015625, ((1, 2),)),
        "w_value_up": bell_draw(seeds[14], (KV_RANK, HEADS * VDIM), KV_RANK ** -0.5, 0.25, ((1, 2),)),
        "ctx_bias": jnp.clip(2.0 + 1.5 * jax.random.uniform(seeds[15], (HEADS,), jnp.float32) ** steps_of(seeds[15], (HEADS,), ((0, 2),), -0.2, 0.2), 2.0, 3.5),
        "w_out": bell_draw(seeds[16], (HEADS * VDIM, D), (4.0 * (HEADS * VDIM) ** -0.5), 0.52734375, ((0, 2),)),
    }


EPS = 1e-06
ROPE_BASE = 10000.0

def modulate(rows_in, gain, shift, scale):
    values = rows_in.astype(jnp.float32)
    normed = values * lax.rsqrt(lax.optimization_barrier(jnp.mean(values * values, axis=-1, keepdims=True)) + EPS)
    return (normed * gain * (1.0 + scale) + shift).astype(jnp.bfloat16)

def compress(rows_in, w_kv_down, kv_gain):
    inner = jnp.dot(rows_in, w_kv_down, preferred_element_type=jnp.float32)
    normed = inner * lax.rsqrt(lax.optimization_barrier(jnp.mean(inner * inner, axis=-1, keepdims=True)) + EPS)
    return (normed * kv_gain).astype(jnp.bfloat16)

def angles(positions):
    quarter = ROPE // 4
    inverse = ROPE_BASE ** (-jnp.arange(quarter, dtype=jnp.float32) / quarter)
    row = (positions // GRID_W).astype(jnp.float32)
    column = (positions % GRID_W).astype(jnp.float32)
    return jnp.concatenate([row[:, None] * inverse[None, :], column[:, None] * inverse[None, :]], axis=-1)

def rotate(values, angle):
    pairs = values.reshape(values.shape[:-1] + (values.shape[-1] // 2, 2))
    first = pairs[..., 0]
    second = pairs[..., 1]
    cosine = jnp.cos(angle)
    sine = jnp.sin(angle)
    turned = jnp.stack([first * cosine - second * sine, first * sine + second * cosine], axis=-1)
    return turned.reshape(values.shape)

def reference(latent, cond, ctx_mod, context, shift_w, scale_w, gate_w, norm_gain, w_qn, w_qr, w_kv_down, w_rope_key, kv_gain, w_key_up, w_value_up, ctx_bias, w_out):
    pair = jnp.stack([jax.nn.silu(cond), jax.nn.silu(ctx_mod)])
    shift = jnp.dot(pair, shift_w, precision=lax.Precision.HIGHEST)
    scale = jnp.dot(pair, scale_w, precision=lax.Precision.HIGHEST)
    gate = jnp.dot(pair, gate_w, precision=lax.Precision.HIGHEST)
    h_rows = modulate(latent, norm_gain, shift[0], scale[0])
    h_ctx = modulate(context, norm_gain, shift[1], scale[1])
    turn = angles(jnp.arange(SEQ, dtype=jnp.int32))
    query_nope = jnp.dot(h_rows, w_qn, preferred_element_type=jnp.float32).astype(jnp.bfloat16)
    query_nope = query_nope.reshape(SEQ, HEADS, NOPE)
    query_rope = jnp.dot(h_rows, w_qr, preferred_element_type=jnp.float32).reshape(SEQ, HEADS, ROPE)
    query_rope = rotate(query_rope, turn[:, None, :]).astype(jnp.bfloat16)
    latents = jnp.concatenate([compress(h_rows, w_kv_down, kv_gain), compress(h_ctx, w_kv_down, kv_gain)], axis=0)
    rope_rows = rotate(jnp.dot(h_rows, w_rope_key, preferred_element_type=jnp.float32), turn).astype(jnp.bfloat16)
    rope_ctx = jnp.dot(h_ctx, w_rope_key, preferred_element_type=jnp.float32).astype(jnp.bfloat16)
    rope_keys = jnp.concatenate([rope_rows, rope_ctx], axis=0)
    total_keys = SEQ + CTX
    keys = jnp.dot(latents, w_key_up, preferred_element_type=jnp.float32).astype(jnp.bfloat16)
    keys = keys.reshape(total_keys, HEADS, NOPE).astype(jnp.float32)
    values = jnp.dot(latents, w_value_up, preferred_element_type=jnp.float32).astype(jnp.bfloat16)
    values = values.reshape(total_keys, HEADS, VDIM).astype(jnp.float32)
    rope_wide = rope_keys.astype(jnp.float32)
    is_ctx = jnp.concatenate([jnp.zeros((SEQ,), jnp.float32), jnp.ones((CTX,), jnp.float32)])
    offset = ctx_bias[:, None] * is_ctx[None, :]
    factor = (NOPE + ROPE) ** (-0.5)
    block = 512
    count = SEQ // block

    def attend(pieces):
        nope_block, rope_block = pieces
        scores = jnp.einsum('qhd,khd->hqk', nope_block.astype(jnp.float32), keys)
        scores = scores + jnp.einsum('qhr,kr->hqk', rope_block.astype(jnp.float32), rope_wide)
        scores = scores * factor + offset[:, None, :]
        top = lax.optimization_barrier(jnp.max(scores, axis=-1, keepdims=True))
        weights = jnp.exp(scores - top)
        total = lax.optimization_barrier(jnp.sum(weights, axis=-1))
        rounded = lax.optimization_barrier(weights.astype(jnp.bfloat16))
        mixed_heads = jnp.einsum('hqk,khd->qhd', rounded.astype(jnp.float32), values)
        result = mixed_heads / jnp.transpose(total)[:, :, None]
        return result.reshape(block, HEADS * VDIM).astype(jnp.bfloat16)
    attended = lax.map(attend, (query_nope.reshape(count, block, HEADS, NOPE), query_rope.reshape(count, block, HEADS, ROPE)))
    attended = attended.reshape(SEQ, HEADS * VDIM)
    group = HEADS_DEV * VDIM

    def add_group(index, total):
        part = lax.dynamic_slice_in_dim(attended, index * group, group, 1)
        rows_part = lax.dynamic_slice_in_dim(w_out, index * group, group, 0)
        term = jnp.dot(part, rows_part, preferred_element_type=jnp.float32).astype(jnp.bfloat16)
        term = lax.optimization_barrier(term)
        return total + term.astype(jnp.float32)
    branch = lax.fori_loop(0, N_TP, add_group, jnp.zeros((SEQ, D), jnp.float32))
    return (latent.astype(jnp.float32) + gate[0] * branch).astype(jnp.bfloat16)
```

```python
import functools

import jax
import jax.numpy as jnp
import numpy as np
from jax import lax
from jax.experimental import pallas as pl
from jax.experimental.pallas import tpu as pltpu
from jax.sharding import PartitionSpec as P

GRID_W = 128
EPS = 1e-06
ROPE_BASE = 10000.0
LANES = 128
LOG2E = 1.4426950408889634
MODS = 5
MESH = pl.DeviceIdType.MESH
F32 = jnp.float32
BF16 = jnp.bfloat16


def remote(src, dst, send, recv, device):
    return pltpu.make_async_remote_copy(
        src_ref=src, dst_ref=dst, send_sem=send, recv_sem=recv, device_id=device, device_id_type=MESH
    )


def rotate(values, cosine, sine):
    width = values.shape[-1]
    ahead = pltpu.roll(values, width - 1, 1)
    behind = pltpu.roll(values, 1, 1)
    even = lax.broadcasted_iota(jnp.int32, values.shape, 1) % 2 == 0
    return values * cosine + jnp.where(even, ahead, behind) * sine


def dot(a, b):
    return jnp.dot(a, b, preferred_element_type=F32)


def dot_nt(a, b):
    return lax.dot_general(a, b, (((1,), (1,)), ((), ())), preferred_element_type=F32)


class Slot:
    def __init__(self, rows, ctx_rows, rank):
        self.split = 2 if rows % 32 == 0 else 1
        self.rows = rows
        self.ctx = -(-ctx_rows // 16) * 16
        self.columns = rank // LANES
        self.rope_at = self.columns * rows
        self.rope_rows = rows // self.split
        self.ctx_at = self.rope_at + self.rope_rows
        self.ctx_rope_at = self.ctx_at + self.columns * self.ctx
        self.height = self.ctx_rope_at + self.ctx

    def planes(self, n_tp, nz):
        return max(1, min(nz, 512 // (self.ctx * 4 * n_tp)))


def kernel(
    n_sp, n_tp, heads, nope, rope, ctx_rows, factor, slot_of,
    cond_hbm, ctxm_hbm, shift_hbm, scale_hbm, gate_hbm, latent_hbm, context_hbm, gain_hbm, down_hbm, rope_hbm,
    kvg_hbm, rowtab_hbm, coltab_hbm, bias_hbm, qr_hbm, qn_hbm, ku_hbm, vu_hbm, wo_hbm,
    out_ref,
    cond_v, ctxm_v, shift_v, scale_v, gate_v, x_v, ctx_v, gain_v, down_v, rope_v, kvg_v, rowtab_v, coltab_v, bias_v,
    qr_v, qn_v, ku_v, vu_v, wo_v, load_sem,
    part, landed, reduced, full, mods, normed, hown, hfull, cos_v, sin_v, vut, bias_b,
    buf, qt, kbuf, vt, acc, top, total_v, att, outbox, inbox,
    send1, recv1, send2, recv2, send_x, recv_x, send, recv, send_t, recv_t, send_o, recv_o,
):
    me = lax.axis_index("sp")
    mine = lax.axis_index("tp")
    total = n_sp * n_tp
    flat = me * n_tp + mine
    barrier = pltpu.get_barrier_semaphore()
    rows, rank = slot_of.rows, ku_v.shape[0]
    depth = x_v.shape[2]
    tokens = n_tp * rows
    partners = [lax.rem(mine + i, n_tp) for i in range(1, n_tp)]

    pairs = dict(
        cond=(cond_hbm, cond_v), ctxm=(ctxm_hbm, ctxm_v), shift=(shift_hbm, shift_v), scale=(scale_hbm, scale_v),
        gate=(gate_hbm, gate_v), x=(latent_hbm, x_v.at[mine]), ctx=(context_hbm, ctx_v), gain=(gain_hbm, gain_v),
        down=(down_hbm, down_v), rope=(rope_hbm, rope_v), kvg=(kvg_hbm, kvg_v), rowtab=(rowtab_hbm, rowtab_v),
        coltab=(coltab_hbm, coltab_v), bias=(bias_hbm, bias_v), qr=(qr_hbm, qr_v), qn=(qn_hbm, qn_v),
        ku=(ku_hbm, ku_v), vu=(vu_hbm, vu_v), wo=(wo_hbm, wo_v),
    )
    loads = {
        name: pltpu.make_async_copy(src, dst, load_sem.at[i]) for i, (name, (src, dst)) in enumerate(pairs.items())
    }
    late = ("qr", "qn", "ku", "vu", "wo")
    for name in loads:
        if name not in late:
            loads[name].start()

    part[...] = jnp.zeros_like(part)
    landed[...] = jnp.zeros_like(landed)

    def greet(i, _):
        other = lax.rem(flat + i, total)
        pl.semaphore_signal(barrier, inc=1, device_id=(other // n_tp, other % n_tp), device_id_type=MESH)
        return 0

    lax.fori_loop(1, total, greet, 0)

    feat, columns = shift_v.shape
    blocks = columns // LANES
    per = -(-MODS * blocks // n_sp)
    sides = []
    for name, ref in (("cond", cond_v), ("ctxm", ctxm_v)):
        loads[name].wait()
        value = ref[pl.ds(me, 1), :]
        value = value / (1.0 + jnp.exp(-value))
        sides.append(jnp.broadcast_to(value, (LANES, feat)).T)
    plan = ((shift_v, 0, "shift"), (shift_v, 1, None), (scale_v, 0, "scale"), (scale_v, 1, None), (gate_v, 0, "gate"))
    for row, (weight, which, name) in enumerate(plan):
        if name:
            loads[name].wait()
        for block in range(blocks):
            unit = row * blocks + block
            part[unit // per, unit % per : unit % per + 1, :] = jnp.sum(
                weight[:, block * LANES : (block + 1) * LANES] * sides[which], axis=0, keepdims=True
            )
    for name in late:
        loads[name].start()
    pl.semaphore_wait(barrier, total - 1)

    some = pl.ds(0, per)

    def scattering(other):
        return remote(part.at[other, some], landed.at[me, some], send1.at[other], recv1.at[me], (other, mine))

    def scatter(i, _):
        scattering(lax.rem(me + i, n_sp)).start()
        return 0

    lax.fori_loop(1, n_sp, scatter, 0)
    loads["x"].wait()
    swaps = [remote(x_v.at[mine], x_v.at[mine], send_x.at[t], recv_x.at[mine], (me, t)) for t in partners]
    for swap in swaps:
        swap.start()
    landed[me] = part[me]

    loads["gain"].wait()
    loads["ctx"].wait()
    gain = gain_v[...]

    def norm(values):
        values = values.astype(F32)
        return values * lax.rsqrt(jnp.mean(values * values, axis=-1, keepdims=True) + EPS) * gain

    ctx = slot_of.ctx
    normed[:rows] = norm(x_v[mine])
    padded = ctx_v[...]
    if ctx != ctx_rows:
        padded = jnp.concatenate([padded.astype(F32), jnp.zeros((ctx - ctx_rows, depth), F32)], axis=0)
    normed[rows:] = norm(padded)

    loads["rowtab"].wait()
    loads["coltab"].wait()
    for k in range(tokens // GRID_W):
        line = pl.ds(me * (tokens // GRID_W) + k, 1)
        at = slice(k * GRID_W, (k + 1) * GRID_W)
        cos_v[at] = coltab_v[0] + rowtab_v[0, line]
        sin_v[at] = coltab_v[1] + rowtab_v[1, line]

    def scattered(i, _):
        other = lax.rem(me + i, n_sp)
        remote(part.at[other, some], landed.at[other, some], send1.at[other], recv1.at[other], (other, mine)).wait()
        return 0

    lax.fori_loop(1, n_sp, scattered, 0)
    reduced[...] = jnp.sum(landed[...], axis=0)

    def gather(i, _):
        other = lax.rem(flat + i, total)
        remote(
            reduced.at[some], full.at[flat, some], send2.at[other], recv2.at[flat], (other // n_tp, other % n_tp)
        ).start()
        return 0

    lax.fori_loop(1, total, gather, 0)
    full[flat] = reduced[...]

    loads["vu"].wait()
    for at in range(0, vu_v.shape[1], LANES):
        vut[at : at + LANES, :] = vu_v[:, at : at + LANES].T
    loads["bias"].wait()
    for head in range(heads):
        bias_b[head] = jnp.broadcast_to(bias_v[:, head : head + 1] * LOG2E, bias_b.shape[1:])
    acc[...] = jnp.zeros_like(acc)
    top[...] = jnp.full(top.shape, -1e30, F32)
    total_v[...] = jnp.zeros_like(total_v)
    loads["down"].wait()
    loads["rope"].wait()
    loads["kvg"].wait()

    def gathered(i, _):
        other = lax.rem(flat + i, total)
        remote(
            reduced.at[some], full.at[other, some], send2.at[other], recv2.at[other], (other // n_tp, other % n_tp)
        ).wait()
        return 0

    lax.fori_loop(1, total, gathered, 0)
    for unit in range(MODS * blocks):
        row, block = unit // blocks, unit % blocks
        for t in range(n_tp):
            at = t * columns + block * LANES
            mods[row : row + 1, at : at + LANES] = full[(unit // per) * n_tp + t, unit % per : unit % per + 1, :]

    def modulate(values, which):
        return (values * (1.0 + mods[2 + which : 3 + which, :]) + mods[which : which + 1, :]).astype(BF16)

    hown[:rows] = modulate(normed[:rows], 0)
    hown[rows:] = modulate(normed[rows:], 1)
    h = hown[...]
    inner = dot(h, down_v[...])
    inner = inner * lax.rsqrt(jnp.mean(inner * inner, axis=-1, keepdims=True) + EPS)
    inner = (inner * kvg_v[...]).astype(BF16)
    key = dot_nt(h, rope_v[...])
    key = jnp.concatenate([key, jnp.zeros((key.shape[0], LANES - rope), F32)], axis=1)
    own_rows = pl.ds(pl.multiple_of(mine * rows, rows), rows)
    turned = rotate(key[:rows], cos_v[own_rows], sin_v[own_rows])

    nz = n_sp // 4
    z, side = me // 4, me % 4
    y, x = side // 2, side % 2
    odd = mine % 2
    flip_x = y * 2 + (1 - x)
    flip_y = (1 - y) * 2 + x
    side_a = flip_x * (1 - odd) + flip_y * odd
    side_b = flip_y * (1 - odd) + flip_x * odd
    side_ab = 3 - side

    own = (mine, z, side)
    for c in range(slot_of.columns):
        lanes = slice(c * LANES, (c + 1) * LANES)
        buf[mine, z, side, c * rows : (c + 1) * rows] = inner[:rows, lanes]
        at = slot_of.ctx_at + c * ctx
        buf[mine, z, side, at : at + ctx] = inner[rows:, lanes]
    shared = turned[: slot_of.rope_rows]
    if slot_of.split == 2:
        shared = shared + pltpu.roll(turned[slot_of.rope_rows :], rope, 1)
    buf[mine, z, side, slot_of.rope_at : slot_of.ctx_at] = shared.astype(BF16)
    buf[mine, z, side, slot_of.ctx_rope_at :] = key[rows:].astype(BF16)

    def plane(step, t):
        sign = 1 - 2 * (1 - t % 2)
        reach = jnp.minimum(z, nz - 1 - z)
        away = (step + 1) // 2
        near = z + (2 * (step % 2) - 1) * sign * away
        low = z <= nz - 1 - z
        far = lax.select(low, z * 0 + step, z * 0 + (nz - 1) - step)
        return lax.select(reach * 2 >= step, near, far)

    def slot(t, zz, ss):
        return buf.at[t, zz, ss]

    def peer(zz, ss):
        return (zz * 4 + ss, mine)

    def link(zz, ss, way, device):
        return remote(slot(mine, zz, ss), slot(mine, zz, ss), send.at[way, zz, ss], recv.at[zz, ss], device)

    def push(zz, ss, way, device, when=None):
        if when is None:
            link(zz, ss, way, device).start()
        else:
            pl.when(when)(lambda: link(zz, ss, way, device).start())

    def pushed(zz, ss, way, when=None):
        wait = lambda: link(zz, ss, way, peer(z, side_a)).wait_send()
        if when is None:
            wait()
        else:
            pl.when(when)(wait)

    def over(zz, ss, t):
        return remote(slot(mine, zz, ss), slot(mine, zz, ss), send_t.at[t, zz, ss], recv_t.at[mine, zz, ss], (me, t))

    def across(zz, ss):
        for t in partners:
            over(zz, ss, t).start()

    def arrived(zz, ss):
        link(zz, ss, 0, peer(z, side_a)).wait_recv()

    up, down = peer(lax.rem(z + 1, nz), side), peer(lax.rem(z + nz - 1, nz), side)
    to_a, to_b = peer(z, side_a), peer(z, side_b)

    def event_z(step):
        zz = plane(step, mine)
        if step == 0:
            push(zz, side, 3, to_b)
            push(zz, side, 2, to_a)
            push(zz, side, 0, up, z < nz - 1)
            push(zz, side, 1, down, z > 0)
        else:
            arrived(zz, side)
            push(zz, side, 0, up, (zz < z) & (z < nz - 1))
            push(zz, side, 1, down, (zz > z) & (z > 0))
            push(zz, side, 2, to_a)
            push(zz, side, 3, to_b)
        across(zz, side)

    def event_a(step):
        zz = plane(step, mine)
        arrived(zz, side_a)
        push(zz, side_a, 3, to_b)
        across(zz, side_a)

    def event_b(step, which):
        zz = plane(step, mine)
        arrived(zz, which)
        across(zz, which)

    def sent():
        for step in range(nz):
            zz = plane(step, mine)
            pushed(zz, side, 2)
            pushed(zz, side, 3)
            pushed(zz, side_a, 3)
            pushed(zz, side, 0, (zz <= z) & (z < nz - 1))
            pushed(zz, side, 1, (zz >= z) & (z > 0))
            for ss in (side, side_a, side_b, side_ab):
                for t in partners:
                    over(zz, ss, t).wait_send()

    event_z(0)

    hfull[mine] = hown[:rows]
    for t in partners:
        remote(x_v.at[t], x_v.at[t], send_x.at[t], recv_x.at[t], (me, t)).wait_recv()
        hfull[t] = modulate(norm(x_v[t]), 0)
    piece = hfull[...].reshape(tokens, depth)
    loads["qr"].wait()
    turned = dot(piece, qr_v[...])
    copies = turned.shape[1] // LANES
    turned = rotate(turned, jnp.concatenate([cos_v[...]] * copies, axis=1), jnp.concatenate([sin_v[...]] * copies, axis=1))
    turned = (turned * (factor * LOG2E)).T.astype(BF16)
    blank = jnp.zeros((LANES - rope, tokens), BF16)
    for head in range(heads):
        mine_rope = turned[head * rope : (head + 1) * rope]
        for g in range(slot_of.split):
            both = [mine_rope, blank] if g == 0 else [blank, mine_rope]
            qt[head, g, nope:, :] = jnp.concatenate(both, axis=0)
    loads["qn"].wait()
    wide = min(2 * nope, heads * nope)
    for at in range(0, heads * nope, wide):
        flatq = dot(piece, qn_v[:, at : at + wide]) * (factor * LOG2E)
        for k in range(wide // nope):
            value = flatq[:, k * nope : (k + 1) * nope].T.astype(BF16)
            for g in range(slot_of.split):
                qt[at // nope + k, g, :nope, :] = value
    loads["ku"].wait()

    def process(lat, ropes, biased=False, valid=None):
        count = lat.shape[0]
        piece_rows = count // len(ropes)
        for at in range(0, heads * nope, wide):
            kbuf[:count, at : at + wide] = dot(lat, ku_v[:, at : at + wide]).astype(BF16)
            vt[at : at + wide, :count] = dot_nt(vut[at : at + wide, :], lat).astype(BF16)
        for head in range(heads):
            pieces = []
            for g, rope_rows in enumerate(ropes):
                keys = jnp.concatenate(
                    [kbuf[g * piece_rows : (g + 1) * piece_rows, head * nope : (head + 1) * nope], rope_rows], axis=1
                )
                pieces.append(dot(keys, qt[head, g]))
            scores = jnp.concatenate(pieces, axis=0)
            if valid is not None:
                scores = jnp.where(valid, scores, -1e30)
            old = top[head][:1]
            high = jnp.max(scores, axis=0, keepdims=True)
            if biased:
                high = high + bias_b[head][:1]
            new = jnp.maximum(old, high)
            less = new - bias_b[head][:1] if biased else new
            weights = jnp.exp2(scores - less)
            fade = jnp.exp2(old - new)
            top[head] = jnp.broadcast_to(new, top.shape[1:])
            total_v[head] = total_v[head] * fade + jnp.sum(weights, axis=0, keepdims=True)
            acc[head] = acc[head] * fade + dot(vt[head * nope : (head + 1) * nope, :count], weights.astype(BF16))

    def chunk(k):
        step, half = k // 2, k % 2
        pair = (
            jnp.where(half == 0, side, flip_y),
            jnp.where(half == 0, flip_x, side_ab),
        )
        places = [(t, plane(step, t), ss) for t in range(n_tp) for ss in pair]
        for t in partners:
            zz = plane(step, t)
            for ss in pair:
                remote(slot(t, zz, ss), slot(t, zz, ss), send_t.at[t, zz, ss], recv_t.at[t, zz, ss], (me, t)).wait_recv()
        tall = slot_of.rope_rows

        def block(place, c, g):
            t, zz, ss = place
            return buf[t, zz, ss, c * rows + g * tall : c * rows + (g + 1) * tall]

        lat = jnp.concatenate(
            [
                jnp.concatenate([block(place, c, g) for g in range(slot_of.split) for place in places], axis=0)
                for c in range(slot_of.columns)
            ],
            axis=1,
        )
        ropes = jnp.concatenate(
            [buf[t, zz, ss, slot_of.rope_at : slot_of.ctx_at] for t, zz, ss in places], axis=0
        )
        process(lat, [ropes] * slot_of.split)

    def before(k):
        if k < nz:
            event_a(k)
        if k + 1 < nz:
            event_z(k + 1)
        event_b(k // 2, side_b if k % 2 == 0 else side_ab)

    def turn(k, _):
        for i in range(2 * nz):
            pl.when(k == i)(functools.partial(before, i))
        chunk(k)
        return 0

    lax.fori_loop(0, 2 * nz, turn, 0)

    per_plane = slot_of.planes(n_tp, nz)

    def context_chunk(i, _):
        places = [
            (t, i * per_plane + dz, ss) for t in range(n_tp) for dz in range(per_plane) for ss in range(4)
        ]
        lat = jnp.concatenate(
            [
                jnp.concatenate(
                    [
                        buf[t, zz, ss, slot_of.ctx_at + c * ctx : slot_of.ctx_at + (c + 1) * ctx]
                        for t, zz, ss in places
                    ],
                    axis=0,
                )
                for c in range(slot_of.columns)
            ],
            axis=1,
        )
        ropes = jnp.concatenate([buf[t, zz, ss, slot_of.ctx_rope_at :] for t, zz, ss in places], axis=0)
        valid = None
        if ctx != ctx_rows:
            valid = lax.broadcasted_iota(jnp.int32, (lat.shape[0], tokens), 0) % ctx < ctx_rows
        process(lat, [ropes], True, valid)
        return 0

    if nz // per_plane == 1:
        context_chunk(0, 0)
    else:
        lax.fori_loop(0, nz // per_plane, context_chunk, 0)

    for head in range(heads):
        att[:, head * nope : (head + 1) * nope] = (acc[head] / total_v[head][:1]).T.astype(BF16)
    loads["wo"].wait()
    shipped = []
    for t in partners:
        lines = pl.ds(pl.multiple_of(t * rows, rows), rows)
        outbox[t] = dot(att[lines, :], wo_v[...]).astype(BF16)
        copy = remote(outbox.at[t], inbox.at[mine], send_o.at[t], recv_o.at[mine], (me, t))
        copy.start()
        shipped.append(copy)
    branch = dot(att[own_rows, :], wo_v[...]).astype(BF16).astype(F32)
    for t in partners:
        remote(outbox.at[t], inbox.at[t], send_o.at[t], recv_o.at[t], (me, t)).wait_recv()
        branch = branch + inbox[t].astype(F32)
    out_ref[...] = (x_v[mine].astype(F32) + mods[4:5, :] * branch).astype(BF16)
    for copy in swaps + shipped:
        copy.wait_send()
    sent()


def tables(count, rope):
    quarter = rope // 4
    lane = np.arange(LANES)
    pair = (lane % rope) // 2
    inverse = (np.float32(ROPE_BASE) ** (-(pair % quarter).astype(np.float32) / np.float32(quarter))).astype(np.float32)
    is_row = (pair < quarter)[None, :]
    out = []
    for size, keep in ((count, is_row), (GRID_W, ~is_row)):
        angle = (np.arange(size, dtype=np.float32)[:, None] * inverse[None, :]).astype(np.float32)
        sine = np.sin(angle)
        signed = np.where(lane[None, :] % 2 == 0, -sine, sine)
        out.append(np.stack([np.where(keep, np.cos(angle), 0.0), np.where(keep, signed, 0.0)]).astype(np.float32))
    return out


def body(
    latent, cond, ctx_mod, context, shift_w, scale_w, gate_w, norm_gain, w_qn, w_qr, w_kv_down, w_rope_key,
    kv_gain, w_key_up, w_value_up, ctx_bias, w_out,
):
    n_sp, n_tp = lax.axis_size("sp"), lax.axis_size("tp")
    rows, width = latent.shape
    ctx_rows = context.shape[0]
    tokens = rows * n_tp
    heads = ctx_bias.shape[0]
    nope = w_key_up.shape[1] // heads
    rope = w_rope_key.shape[1]
    rank = w_kv_down.shape[1]
    factor = (nope + rope) ** (-0.5)
    feat, columns = shift_w.shape
    slot_of = Slot(rows, ctx_rows, rank)
    nz = n_sp // 4
    short = -(heads * rope) % LANES
    if short:
        w_qr = jnp.concatenate([w_qr, jnp.zeros((width, short), BF16)], axis=1)
    rowtab, coltab = tables(tokens * n_sp // GRID_W, rope)
    chunk_rows = n_tp * max(2 * rows, 4 * slot_of.ctx * slot_of.planes(n_tp, nz))

    def like(a):
        return pltpu.VMEM(a.shape, a.dtype)

    operands = (
        cond.reshape(n_sp, feat), ctx_mod.reshape(n_sp, feat), shift_w, scale_w, gate_w, latent, context,
        norm_gain[None, :], w_kv_down, w_rope_key.T, kv_gain[None, :], rowtab, coltab, ctx_bias[None, :],
        w_qr, w_qn, w_key_up, w_value_up, w_out,
    )
    staged = [like(a) for a in operands]
    staged[5] = pltpu.VMEM((n_tp, rows, width), BF16)
    dma = pltpu.SemaphoreType.DMA
    return pl.pallas_call(
        functools.partial(kernel, n_sp, n_tp, heads, nope, rope, ctx_rows, factor, slot_of),
        out_shape=jax.ShapeDtypeStruct((rows, width), BF16),
        in_specs=[pl.BlockSpec(memory_space=pl.ANY)] * len(operands),
        out_specs=pl.BlockSpec(memory_space=pltpu.VMEM),
        scratch_shapes=staged + [
            dma((len(operands),)),
            pltpu.VMEM((n_sp, 8, LANES), F32),
            pltpu.VMEM((n_sp, 8, LANES), F32),
            pltpu.VMEM((8, LANES), F32),
            pltpu.VMEM((n_sp * n_tp, 8, LANES), F32),
            pltpu.VMEM((8, width), F32),
            pltpu.VMEM((rows + slot_of.ctx, width), F32),
            pltpu.VMEM((rows + slot_of.ctx, width), BF16),
            pltpu.VMEM((n_tp, rows, width), BF16),
            pltpu.VMEM((tokens, LANES), F32),
            pltpu.VMEM((tokens, LANES), F32),
            pltpu.VMEM((w_value_up.shape[1], rank), BF16),
            pltpu.VMEM((heads, 8, tokens), F32),
            pltpu.VMEM((n_tp, nz, 4, slot_of.height, LANES), BF16),
            pltpu.VMEM((heads, slot_of.split, nope + LANES, tokens), BF16),
            pltpu.VMEM((chunk_rows, heads * nope), BF16),
            pltpu.VMEM((heads * nope, chunk_rows), BF16),
            pltpu.VMEM((heads, nope, tokens), F32),
            pltpu.VMEM((heads, 8, tokens), F32),
            pltpu.VMEM((heads, 8, tokens), F32),
            pltpu.VMEM((tokens, heads * nope), BF16),
            pltpu.VMEM((n_tp, rows, width), BF16),
            pltpu.VMEM((n_tp, rows, width), BF16),
            dma((n_sp,)),
            dma((n_sp,)),
            dma((n_sp * n_tp,)),
            dma((n_sp * n_tp,)),
            dma((n_tp,)),
            dma((n_tp,)),
            dma((4, nz, 4)),
            dma((nz, 4)),
            dma((n_tp, nz, 4)),
            dma((n_tp, nz, 4)),
            dma((n_tp,)),
            dma((n_tp,)),
        ],
        compiler_params=pltpu.CompilerParams(
            collective_id=0, has_side_effects=True, vmem_limit_bytes=62 * 1024 * 1024
        ),
        name="block",
    )(*operands)


def solution(mesh):
    placed = (
        P(("sp", "tp"), None),
        P(),
        P(),
        P(("sp", "tp"), None),
        P("sp", "tp"),
        P("sp", "tp"),
        P("sp", "tp"),
        P(),
        P(None, "tp"),
        P(None, "tp"),
        P(),
        P(),
        P(),
        P(None, "tp"),
        P(None, "tp"),
        P("tp"),
        P("tp", None),
    )
    return jax.shard_map(
        body, mesh=mesh, in_specs=placed, out_specs=P(("sp", "tp"), None), check_vma=False
    )
```

```python
import functools

import jax
import jax.numpy as jnp
import numpy as np
from jax import lax
from jax.experimental import pallas as pl
from jax.experimental.pallas import tpu as pltpu
from jax.sharding import PartitionSpec as P

GRID_W = 128
EPS = 1e-06
ROPE_BASE = 10000.0
LANES = 128
LOG2E = 1.4426950408889634
MODS = 5
MESH = pl.DeviceIdType.MESH
F32 = jnp.float32
BF16 = jnp.bfloat16


def remote(src, dst, send, recv, device):
    return pltpu.make_async_remote_copy(
        src_ref=src, dst_ref=dst, send_sem=send, recv_sem=recv, device_id=device, device_id_type=MESH
    )


def rotate(values, cosine, sine):
    width = values.shape[-1]
    ahead = pltpu.roll(values, width - 1, 1)
    behind = pltpu.roll(values, 1, 1)
    even = lax.broadcasted_iota(jnp.int32, values.shape, 1) % 2 == 0
    return values * cosine + jnp.where(even, ahead, behind) * sine


def dot(a, b):
    return jnp.dot(a, b, preferred_element_type=F32)


def dot_nt(a, b):
    return lax.dot_general(a, b, (((1,), (1,)), ((), ())), preferred_element_type=F32)


class Slot:
    def __init__(self, rows, ctx_rows, rank):
        self.split = 2 if rows % 32 == 0 else 1
        self.rows = rows
        self.ctx = -(-ctx_rows // 16) * 16
        self.columns = rank // LANES
        self.rope_at = self.columns * rows
        self.rope_rows = rows // self.split
        self.ctx_at = self.rope_at + self.rope_rows
        self.ctx_rope_at = self.ctx_at + self.columns * self.ctx
        self.height = self.ctx_rope_at + self.ctx

    def planes(self, n_tp, nz):
        return max(1, min(nz, 512 // (self.ctx * 4 * n_tp)))


def kernel(
    n_sp, n_tp, heads, nope, rope, ctx_rows, factor, slot_of,
    cond_hbm, ctxm_hbm, shift_hbm, scale_hbm, gate_hbm, latent_hbm, context_hbm, gain_hbm, down_hbm, rope_hbm,
    kvg_hbm, rowtab_hbm, coltab_hbm, bias_hbm, qr_hbm, qn_hbm, ku_hbm, vu_hbm, wo_hbm,
    out_ref,
    cond_v, ctxm_v, shift_v, scale_v, gate_v, x_v, ctx_v, gain_v, down_v, rope_v, kvg_v, rowtab_v, coltab_v, bias_v,
    qr_v, qn_v, ku_v, vu_v, wo_v, load_sem,
    part, landed, reduced, full, mods, normed, hown, hfull, cos_v, sin_v, vut, bias_b,
    buf, qt, kbuf, vt, sbuf, acc, top, total_v, att, outbox, inbox,
    send1, recv1, send2, recv2, send_x, recv_x, send, recv, send_t, recv_t, send_o, recv_o,
):
    me = lax.axis_index("sp")
    mine = lax.axis_index("tp")
    total = n_sp * n_tp
    flat = me * n_tp + mine
    barrier = pltpu.get_barrier_semaphore()
    rows, rank = slot_of.rows, ku_v.shape[0]
    depth = x_v.shape[2]
    tokens = n_tp * rows
    partners = [lax.rem(mine + i, n_tp) for i in range(1, n_tp)]

    pairs = dict(
        cond=(cond_hbm, cond_v), ctxm=(ctxm_hbm, ctxm_v), shift=(shift_hbm, shift_v), scale=(scale_hbm, scale_v),
        gate=(gate_hbm, gate_v), x=(latent_hbm, x_v.at[mine]), ctx=(context_hbm, ctx_v), gain=(gain_hbm, gain_v),
        down=(down_hbm, down_v), rope=(rope_hbm, rope_v), kvg=(kvg_hbm, kvg_v), rowtab=(rowtab_hbm, rowtab_v),
        coltab=(coltab_hbm, coltab_v), bias=(bias_hbm, bias_v), qr=(qr_hbm, qr_v), qn=(qn_hbm, qn_v),
        ku=(ku_hbm, ku_v), vu=(vu_hbm, vu_v), wo=(wo_hbm, wo_v),
    )
    loads = {
        name: pltpu.make_async_copy(src, dst, load_sem.at[i]) for i, (name, (src, dst)) in enumerate(pairs.items())
    }
    late = ("qr", "qn", "ku", "vu", "wo")
    for name in loads:
        if name not in late:
            loads[name].start()

    part[...] = jnp.zeros_like(part)
    landed[...] = jnp.zeros_like(landed)

    def greet(i, _):
        other = lax.rem(flat + i, total)
        pl.semaphore_signal(barrier, inc=1, device_id=(other // n_tp, other % n_tp), device_id_type=MESH)
        return 0

    lax.fori_loop(1, total, greet, 0)

    feat, columns = shift_v.shape
    blocks = columns // LANES
    per = -(-MODS * blocks // n_sp)
    sides = []
    for name, ref in (("cond", cond_v), ("ctxm", ctxm_v)):
        loads[name].wait()
        value = ref[pl.ds(me, 1), :]
        value = value / (1.0 + jnp.exp(-value))
        sides.append(jnp.broadcast_to(value, (LANES, feat)).T)
    plan = ((shift_v, 0, "shift"), (shift_v, 1, None), (scale_v, 0, "scale"), (scale_v, 1, None), (gate_v, 0, "gate"))
    for row, (weight, which, name) in enumerate(plan):
        if name:
            loads[name].wait()
        for block in range(blocks):
            unit = row * blocks + block
            part[unit // per, unit % per : unit % per + 1, :] = jnp.sum(
                weight[:, block * LANES : (block + 1) * LANES] * sides[which], axis=0, keepdims=True
            )
    for name in late:
        loads[name].start()
    pl.semaphore_wait(barrier, total - 1)

    some = pl.ds(0, per)

    def scattering(other):
        return remote(part.at[other, some], landed.at[me, some], send1.at[other], recv1.at[me], (other, mine))

    def scatter(i, _):
        scattering(lax.rem(me + i, n_sp)).start()
        return 0

    lax.fori_loop(1, n_sp, scatter, 0)
    loads["x"].wait()
    swaps = [remote(x_v.at[mine], x_v.at[mine], send_x.at[t], recv_x.at[mine], (me, t)) for t in partners]
    for swap in swaps:
        swap.start()
    landed[me] = part[me]

    loads["gain"].wait()
    loads["ctx"].wait()
    gain = gain_v[...]

    def norm(values):
        values = values.astype(F32)
        return values * lax.rsqrt(jnp.mean(values * values, axis=-1, keepdims=True) + EPS) * gain

    ctx = slot_of.ctx
    normed[:rows] = norm(x_v[mine])
    padded = ctx_v[...]
    if ctx != ctx_rows:
        padded = jnp.concatenate([padded.astype(F32), jnp.zeros((ctx - ctx_rows, depth), F32)], axis=0)
    normed[rows:] = norm(padded)

    loads["rowtab"].wait()
    loads["coltab"].wait()
    for k in range(tokens // GRID_W):
        line = pl.ds(me * (tokens // GRID_W) + k, 1)
        at = slice(k * GRID_W, (k + 1) * GRID_W)
        cos_v[at] = coltab_v[0] + rowtab_v[0, line]
        sin_v[at] = coltab_v[1] + rowtab_v[1, line]

    def scattered(i, _):
        other = lax.rem(me + i, n_sp)
        remote(part.at[other, some], landed.at[other, some], send1.at[other], recv1.at[other], (other, mine)).wait()
        return 0

    lax.fori_loop(1, n_sp, scattered, 0)
    reduced[...] = jnp.sum(landed[...], axis=0)

    def gather(i, _):
        other = lax.rem(flat + i, total)
        remote(
            reduced.at[some], full.at[flat, some], send2.at[other], recv2.at[flat], (other // n_tp, other % n_tp)
        ).start()
        return 0

    lax.fori_loop(1, total, gather, 0)
    full[flat] = reduced[...]

    loads["vu"].wait()
    for at in range(0, vu_v.shape[1], LANES):
        vut[at : at + LANES, :] = vu_v[:, at : at + LANES].T
    loads["bias"].wait()
    for head in range(heads):
        bias_b[head] = jnp.broadcast_to(bias_v[:, head : head + 1] * LOG2E, bias_b.shape[1:])
    acc[...] = jnp.zeros_like(acc)
    top[...] = jnp.full(top.shape, -1e30, F32)
    total_v[...] = jnp.zeros_like(total_v)
    loads["down"].wait()
    loads["rope"].wait()
    loads["kvg"].wait()

    def gathered(i, _):
        other = lax.rem(flat + i, total)
        remote(
            reduced.at[some], full.at[other, some], send2.at[other], recv2.at[other], (other // n_tp, other % n_tp)
        ).wait()
        return 0

    lax.fori_loop(1, total, gathered, 0)
    for unit in range(MODS * blocks):
        row, block = unit // blocks, unit % blocks
        for t in range(n_tp):
            at = t * columns + block * LANES
            mods[row : row + 1, at : at + LANES] = full[(unit // per) * n_tp + t, unit % per : unit % per + 1, :]

    def modulate(values, which):
        return (values * (1.0 + mods[2 + which : 3 + which, :]) + mods[which : which + 1, :]).astype(BF16)

    hown[:rows] = modulate(normed[:rows], 0)
    hown[rows:] = modulate(normed[rows:], 1)
    h = hown[...]
    inner = dot(h, down_v[...])
    inner = inner * lax.rsqrt(jnp.mean(inner * inner, axis=-1, keepdims=True) + EPS)
    inner = (inner * kvg_v[...]).astype(BF16)
    key = dot_nt(h, rope_v[...])
    key = jnp.concatenate([key, jnp.zeros((key.shape[0], LANES - rope), F32)], axis=1)
    own_rows = pl.ds(pl.multiple_of(mine * rows, rows), rows)
    turned = rotate(key[:rows], cos_v[own_rows], sin_v[own_rows])

    nz = n_sp // 4
    z, side = me // 4, me % 4
    y, x = side // 2, side % 2
    odd = mine % 2
    flip_x = y * 2 + (1 - x)
    flip_y = (1 - y) * 2 + x
    side_a = flip_x * (1 - odd) + flip_y * odd
    side_b = flip_y * (1 - odd) + flip_x * odd
    side_ab = 3 - side

    own = (mine, z, side)
    for c in range(slot_of.columns):
        lanes = slice(c * LANES, (c + 1) * LANES)
        buf[mine, z, side, c * rows : (c + 1) * rows] = inner[:rows, lanes]
        at = slot_of.ctx_at + c * ctx
        buf[mine, z, side, at : at + ctx] = inner[rows:, lanes]
    shared = turned[: slot_of.rope_rows]
    if slot_of.split == 2:
        shared = shared + pltpu.roll(turned[slot_of.rope_rows :], rope, 1)
    buf[mine, z, side, slot_of.rope_at : slot_of.ctx_at] = shared.astype(BF16)
    buf[mine, z, side, slot_of.ctx_rope_at :] = key[rows:].astype(BF16)

    def plane(step, t):
        sign = 1 - 2 * (1 - t % 2)
        reach = jnp.minimum(z, nz - 1 - z)
        away = (step + 1) // 2
        near = z + (2 * (step % 2) - 1) * sign * away
        low = z <= nz - 1 - z
        far = lax.select(low, z * 0 + step, z * 0 + (nz - 1) - step)
        return lax.select(reach * 2 >= step, near, far)

    def slot(t, zz, ss):
        return buf.at[t, zz, ss]

    def peer(zz, ss):
        return (zz * 4 + ss, mine)

    def link(zz, ss, way, device):
        return remote(slot(mine, zz, ss), slot(mine, zz, ss), send.at[way, zz, ss], recv.at[zz, ss], device)

    def push(zz, ss, way, device, when=None):
        if when is None:
            link(zz, ss, way, device).start()
        else:
            pl.when(when)(lambda: link(zz, ss, way, device).start())

    def pushed(zz, ss, way, when=None):
        wait = lambda: link(zz, ss, way, peer(z, side_a)).wait_send()
        if when is None:
            wait()
        else:
            pl.when(when)(wait)

    def over(zz, ss, t):
        return remote(slot(mine, zz, ss), slot(mine, zz, ss), send_t.at[t, zz, ss], recv_t.at[mine, zz, ss], (me, t))

    def across(zz, ss):
        for t in partners:
            over(zz, ss, t).start()

    def arrived(zz, ss):
        link(zz, ss, 0, peer(z, side_a)).wait_recv()

    up, down = peer(lax.rem(z + 1, nz), side), peer(lax.rem(z + nz - 1, nz), side)
    to_a, to_b = peer(z, side_a), peer(z, side_b)

    def event_z(step):
        zz = plane(step, mine)
        if step == 0:
            push(zz, side, 3, to_b)
            push(zz, side, 2, to_a)
            push(zz, side, 0, up, z < nz - 1)
            push(zz, side, 1, down, z > 0)
        else:
            arrived(zz, side)
            push(zz, side, 0, up, (zz < z) & (z < nz - 1))
            push(zz, side, 1, down, (zz > z) & (z > 0))
            push(zz, side, 2, to_a)
            push(zz, side, 3, to_b)
        across(zz, side)

    def event_a(step):
        zz = plane(step, mine)
        arrived(zz, side_a)
        push(zz, side_a, 3, to_b)
        across(zz, side_a)

    def event_b(step, which):
        zz = plane(step, mine)
        arrived(zz, which)
        across(zz, which)

    def sent():
        for step in range(nz):
            zz = plane(step, mine)
            pushed(zz, side, 2)
            pushed(zz, side, 3)
            pushed(zz, side_a, 3)
            pushed(zz, side, 0, (zz <= z) & (z < nz - 1))
            pushed(zz, side, 1, (zz >= z) & (z > 0))
            for ss in (side, side_a, side_b, side_ab):
                for t in partners:
                    over(zz, ss, t).wait_send()

    event_z(0)

    hfull[mine] = hown[:rows]
    for t in partners:
        remote(x_v.at[t], x_v.at[t], send_x.at[t], recv_x.at[t], (me, t)).wait_recv()
        hfull[t] = modulate(norm(x_v[t]), 0)
    piece = hfull[...].reshape(tokens, depth)
    loads["qr"].wait()
    turned = dot(piece, qr_v[...])
    copies = turned.shape[1] // LANES
    turned = rotate(turned, jnp.concatenate([cos_v[...]] * copies, axis=1), jnp.concatenate([sin_v[...]] * copies, axis=1))
    turned = (turned * (factor * LOG2E)).T.astype(BF16)
    blank = jnp.zeros((LANES - rope, tokens), BF16)
    for head in range(heads):
        mine_rope = turned[head * rope : (head + 1) * rope]
        for g in range(slot_of.split):
            both = [mine_rope, blank] if g == 0 else [blank, mine_rope]
            qt[head, g, nope:, :] = jnp.concatenate(both, axis=0)
    loads["qn"].wait()
    wide = min(2 * nope, heads * nope)
    for at in range(0, heads * nope, wide):
        flatq = dot(piece, qn_v[:, at : at + wide]) * (factor * LOG2E)
        for k in range(wide // nope):
            value = flatq[:, k * nope : (k + 1) * nope].T.astype(BF16)
            for g in range(slot_of.split):
                qt[at // nope + k, g, :nope, :] = value
    loads["ku"].wait()

    def process(lat, ropes, biased=False, valid=None):
        count = lat.shape[0]
        tall = count // len(ropes)
        share = wide // nope

        def raise_keys(at):
            kbuf[:count, at : at + wide] = dot(lat, ku_v[:, at : at + wide]).astype(BF16)

        def raise_values(at):
            vt[at : at + wide, :count] = dot_nt(vut[at : at + wide, :], lat).astype(BF16)

        def score(head):
            if head % share == 0:
                raise_keys(head * nope)
            high = None
            for g, shared in enumerate(ropes):
                keys = jnp.concatenate(
                    [kbuf[g * tall : (g + 1) * tall, head * nope : (head + 1) * nope], shared], axis=1
                )
                piece = dot(keys, qt[head, g])
                if valid is not None:
                    piece = jnp.where(valid, piece, -1e30)
                sbuf[head % 2, g * tall : (g + 1) * tall] = piece
                peak = jnp.max(piece, axis=0, keepdims=True)
                high = peak if high is None else jnp.maximum(high, peak)
            return high

        def soften(head, high):
            old = top[head][:1]
            if biased:
                high = high + bias_b[head][:1]
            new = jnp.maximum(old, high)
            less = new - bias_b[head][:1] if biased else new
            weights = jnp.exp2(sbuf[head % 2, :count] - less)
            fade = jnp.exp2(old - new)
            top[head] = jnp.broadcast_to(new, top.shape[1:])
            total_v[head] = total_v[head] * fade + jnp.sum(weights, axis=0, keepdims=True)
            acc[head] = acc[head] * fade + dot(vt[head * nope : (head + 1) * nope, :count], weights.astype(BF16))

        high = score(0)
        raise_values(0)
        for head in range(heads):
            later = score(head + 1) if head + 1 < heads else None
            if head + 1 < heads and (head + 1) % share == 0:
                raise_values((head + 1) * nope)
            soften(head, high)
            high = later

    def chunk(k):
        step, half = k // 2, k % 2
        pair = (
            jnp.where(half == 0, side, flip_y),
            jnp.where(half == 0, flip_x, side_ab),
        )
        places = [(t, plane(step, t), ss) for t in range(n_tp) for ss in pair]
        for t in partners:
            zz = plane(step, t)
            for ss in pair:
                remote(slot(t, zz, ss), slot(t, zz, ss), send_t.at[t, zz, ss], recv_t.at[t, zz, ss], (me, t)).wait_recv()
        tall = slot_of.rope_rows

        def block(place, c, g):
            t, zz, ss = place
            return buf[t, zz, ss, c * rows + g * tall : c * rows + (g + 1) * tall]

        lat = jnp.concatenate(
            [
                jnp.concatenate([block(place, c, g) for g in range(slot_of.split) for place in places], axis=0)
                for c in range(slot_of.columns)
            ],
            axis=1,
        )
        ropes = jnp.concatenate(
            [buf[t, zz, ss, slot_of.rope_at : slot_of.ctx_at] for t, zz, ss in places], axis=0
        )
        process(lat, [ropes] * slot_of.split)

    def before(k):
        if k < nz:
            event_a(k)
        if k + 1 < nz:
            event_z(k + 1)
        event_b(k // 2, side_b if k % 2 == 0 else side_ab)

    def turn(k, _):
        for i in range(2 * nz):
            pl.when(k == i)(functools.partial(before, i))
        chunk(k)
        return 0

    lax.fori_loop(0, 2 * nz, turn, 0)

    per_plane = slot_of.planes(n_tp, nz)

    def context_chunk(i, _):
        places = [
            (t, i * per_plane + dz, ss) for t in range(n_tp) for dz in range(per_plane) for ss in range(4)
        ]
        lat = jnp.concatenate(
            [
                jnp.concatenate(
                    [
                        buf[t, zz, ss, slot_of.ctx_at + c * ctx : slot_of.ctx_at + (c + 1) * ctx]
                        for t, zz, ss in places
                    ],
                    axis=0,
                )
                for c in range(slot_of.columns)
            ],
            axis=1,
        )
        ropes = jnp.concatenate([buf[t, zz, ss, slot_of.ctx_rope_at :] for t, zz, ss in places], axis=0)
        valid = None
        if ctx != ctx_rows:
            valid = lax.broadcasted_iota(jnp.int32, (lat.shape[0], tokens), 0) % ctx < ctx_rows
        process(lat, [ropes], True, valid)
        return 0

    if nz // per_plane == 1:
        context_chunk(0, 0)
    else:
        lax.fori_loop(0, nz // per_plane, context_chunk, 0)

    for head in range(heads):
        att[:, head * nope : (head + 1) * nope] = (acc[head] / total_v[head][:1]).T.astype(BF16)
    loads["wo"].wait()
    shipped = []
    for t in partners:
        lines = pl.ds(pl.multiple_of(t * rows, rows), rows)
        outbox[t] = dot(att[lines, :], wo_v[...]).astype(BF16)
        copy = remote(outbox.at[t], inbox.at[mine], send_o.at[t], recv_o.at[mine], (me, t))
        copy.start()
        shipped.append(copy)
    branch = dot(att[own_rows, :], wo_v[...]).astype(BF16).astype(F32)
    for t in partners:
        remote(outbox.at[t], inbox.at[t], send_o.at[t], recv_o.at[t], (me, t)).wait_recv()
        branch = branch + inbox[t].astype(F32)
    out_ref[...] = (x_v[mine].astype(F32) + mods[4:5, :] * branch).astype(BF16)
    for copy in swaps + shipped:
        copy.wait_send()
    sent()


def tables(count, rope):
    quarter = rope // 4
    lane = np.arange(LANES)
    pair = (lane % rope) // 2
    inverse = (np.float32(ROPE_BASE) ** (-(pair % quarter).astype(np.float32) / np.float32(quarter))).astype(np.float32)
    is_row = (pair < quarter)[None, :]
    out = []
    for size, keep in ((count, is_row), (GRID_W, ~is_row)):
        angle = (np.arange(size, dtype=np.float32)[:, None] * inverse[None, :]).astype(np.float32)
        sine = np.sin(angle)
        signed = np.where(lane[None, :] % 2 == 0, -sine, sine)
        out.append(np.stack([np.where(keep, np.cos(angle), 0.0), np.where(keep, signed, 0.0)]).astype(np.float32))
    return out


def body(
    latent, cond, ctx_mod, context, shift_w, scale_w, gate_w, norm_gain, w_qn, w_qr, w_kv_down, w_rope_key,
    kv_gain, w_key_up, w_value_up, ctx_bias, w_out,
):
    n_sp, n_tp = lax.axis_size("sp"), lax.axis_size("tp")
    rows, width = latent.shape
    ctx_rows = context.shape[0]
    tokens = rows * n_tp
    heads = ctx_bias.shape[0]
    nope = w_key_up.shape[1] // heads
    rope = w_rope_key.shape[1]
    rank = w_kv_down.shape[1]
    factor = (nope + rope) ** (-0.5)
    feat, columns = shift_w.shape
    slot_of = Slot(rows, ctx_rows, rank)
    nz = n_sp // 4
    short = -(heads * rope) % LANES
    if short:
        w_qr = jnp.concatenate([w_qr, jnp.zeros((width, short), BF16)], axis=1)
    rowtab, coltab = tables(tokens * n_sp // GRID_W, rope)
    chunk_rows = n_tp * max(2 * rows, 4 * slot_of.ctx * slot_of.planes(n_tp, nz))

    def like(a):
        return pltpu.VMEM(a.shape, a.dtype)

    operands = (
        cond.reshape(n_sp, feat), ctx_mod.reshape(n_sp, feat), shift_w, scale_w, gate_w, latent, context,
        norm_gain[None, :], w_kv_down, w_rope_key.T, kv_gain[None, :], rowtab, coltab, ctx_bias[None, :],
        w_qr, w_qn, w_key_up, w_value_up, w_out,
    )
    staged = [like(a) for a in operands]
    staged[5] = pltpu.VMEM((n_tp, rows, width), BF16)
    dma = pltpu.SemaphoreType.DMA
    return pl.pallas_call(
        functools.partial(kernel, n_sp, n_tp, heads, nope, rope, ctx_rows, factor, slot_of),
        out_shape=jax.ShapeDtypeStruct((rows, width), BF16),
        in_specs=[pl.BlockSpec(memory_space=pl.ANY)] * len(operands),
        out_specs=pl.BlockSpec(memory_space=pltpu.VMEM),
        scratch_shapes=staged + [
            dma((len(operands),)),
            pltpu.VMEM((n_sp, 8, LANES), F32),
            pltpu.VMEM((n_sp, 8, LANES), F32),
            pltpu.VMEM((8, LANES), F32),
            pltpu.VMEM((n_sp * n_tp, 8, LANES), F32),
            pltpu.VMEM((8, width), F32),
            pltpu.VMEM((rows + slot_of.ctx, width), F32),
            pltpu.VMEM((rows + slot_of.ctx, width), BF16),
            pltpu.VMEM((n_tp, rows, width), BF16),
            pltpu.VMEM((tokens, LANES), F32),
            pltpu.VMEM((tokens, LANES), F32),
            pltpu.VMEM((w_value_up.shape[1], rank), BF16),
            pltpu.VMEM((heads, 8, tokens), F32),
            pltpu.VMEM((n_tp, nz, 4, slot_of.height, LANES), BF16),
            pltpu.VMEM((heads, slot_of.split, nope + LANES, tokens), BF16),
            pltpu.VMEM((chunk_rows, heads * nope), BF16),
            pltpu.VMEM((heads * nope, chunk_rows), BF16),
            pltpu.VMEM((2, chunk_rows, tokens), F32),
            pltpu.VMEM((heads, nope, tokens), F32),
            pltpu.VMEM((heads, 8, tokens), F32),
            pltpu.VMEM((heads, 8, tokens), F32),
            pltpu.VMEM((tokens, heads * nope), BF16),
            pltpu.VMEM((n_tp, rows, width), BF16),
            pltpu.VMEM((n_tp, rows, width), BF16),
            dma((n_sp,)),
            dma((n_sp,)),
            dma((n_sp * n_tp,)),
            dma((n_sp * n_tp,)),
            dma((n_tp,)),
            dma((n_tp,)),
            dma((4, nz, 4)),
            dma((nz, 4)),
            dma((n_tp, nz, 4)),
            dma((n_tp, nz, 4)),
            dma((n_tp,)),
            dma((n_tp,)),
        ],
        compiler_params=pltpu.CompilerParams(
            collective_id=0, has_side_effects=True, vmem_limit_bytes=62 * 1024 * 1024
        ),
        name="block",
    )(*operands)


def solution(mesh):
    placed = (
        P(("sp", "tp"), None),
        P(),
        P(),
        P(("sp", "tp"), None),
        P("sp", "tp"),
        P("sp", "tp"),
        P("sp", "tp"),
        P(),
        P(None, "tp"),
        P(None, "tp"),
        P(),
        P(),
        P(),
        P(None, "tp"),
        P(None, "tp"),
        P("tp"),
        P("tp", None),
    )
    return jax.shard_map(
        body, mesh=mesh, in_specs=placed, out_specs=P(("sp", "tp"), None), check_vma=False
    )
```

```python
import functools

import jax
import jax.numpy as jnp
import numpy as np
from jax import lax
from jax.experimental import pallas as pl
from jax.experimental.pallas import tpu as pltpu
from jax.sharding import PartitionSpec as P

GRID_W = 128
EPS = 1e-06
ROPE_BASE = 10000.0
LANES = 128
LOG2E = 1.4426950408889634
MODS = 5
ORDERS = {
    4: (
        ("a0", "z1", "b0", "z2"), ("d0", "a1", "z3", "b1"), ("a2", "b2"), ("d1",), ("d2", "a3"), ("b3",), ("d3",), (),
    )
}
MESH = pl.DeviceIdType.MESH
F32 = jnp.float32
BF16 = jnp.bfloat16


def remote(src, dst, send, recv, device):
    return pltpu.make_async_remote_copy(
        src_ref=src, dst_ref=dst, send_sem=send, recv_sem=recv, device_id=device, device_id_type=MESH
    )


def rotate(values, cosine, sine):
    width = values.shape[-1]
    ahead = pltpu.roll(values, width - 1, 1)
    behind = pltpu.roll(values, 1, 1)
    even = lax.broadcasted_iota(jnp.int32, values.shape, 1) % 2 == 0
    return values * cosine + jnp.where(even, ahead, behind) * sine


def dot(a, b):
    return jnp.dot(a, b, preferred_element_type=F32)


def dot_nt(a, b):
    return lax.dot_general(a, b, (((1,), (1,)), ((), ())), preferred_element_type=F32)


class Slot:
    def __init__(self, rows, ctx_rows, rank):
        self.split = 2 if rows % 32 == 0 else 1
        self.rows = rows
        self.ctx = -(-ctx_rows // 16) * 16
        self.columns = rank // LANES
        self.rope_at = self.columns * rows
        self.rope_rows = rows // self.split
        self.ctx_at = self.rope_at + self.rope_rows
        self.ctx_rope_at = self.ctx_at + self.columns * self.ctx
        self.height = self.ctx_rope_at + self.ctx

    def planes(self, n_tp, nz):
        return max(1, min(nz, 512 // (self.ctx * 4 * n_tp)))


def kernel(
    n_sp, n_tp, heads, nope, rope, ctx_rows, factor, slot_of,
    cond_hbm, ctxm_hbm, shift_hbm, scale_hbm, gate_hbm, latent_hbm, context_hbm, gain_hbm, down_hbm, rope_hbm,
    kvg_hbm, rowtab_hbm, coltab_hbm, bias_hbm, qr_hbm, qn_hbm, ku_hbm, vu_hbm, wo_hbm,
    out_ref,
    cond_v, ctxm_v, shift_v, scale_v, gate_v, x_v, ctx_v, gain_v, down_v, rope_v, kvg_v, rowtab_v, coltab_v, bias_v,
    qr_v, qn_v, ku_v, vu_v, wo_v, load_sem,
    part, land1, sum1, land2, sum2, land3, mods, normed, hown, hfull, cos_v, sin_v, vut, bias_b,
    buf, qt, kbuf, vt, sbuf, acc, top, total_v, att, outbox, inbox,
    send1, recv1, send2, recv2, send3, recv3, send_x, recv_x, send, recv, send_t, recv_t, send_o, recv_o,
):
    me = lax.axis_index("sp")
    mine = lax.axis_index("tp")
    barrier = pltpu.get_barrier_semaphore()
    rows, rank = slot_of.rows, ku_v.shape[0]
    depth = x_v.shape[2]
    tokens = n_tp * rows
    partners = [lax.rem(mine + i, n_tp) for i in range(1, n_tp)]

    pairs = dict(
        cond=(cond_hbm, cond_v), ctxm=(ctxm_hbm, ctxm_v), shift=(shift_hbm, shift_v), scale=(scale_hbm, scale_v),
        gate=(gate_hbm, gate_v), x=(latent_hbm, x_v.at[mine]), ctx=(context_hbm, ctx_v), gain=(gain_hbm, gain_v),
        down=(down_hbm, down_v), rope=(rope_hbm, rope_v), kvg=(kvg_hbm, kvg_v), rowtab=(rowtab_hbm, rowtab_v),
        coltab=(coltab_hbm, coltab_v), bias=(bias_hbm, bias_v), qr=(qr_hbm, qr_v), qn=(qn_hbm, qn_v),
        ku=(ku_hbm, ku_v), vu=(vu_hbm, vu_v), wo=(wo_hbm, wo_v),
    )
    loads = {
        name: pltpu.make_async_copy(src, dst, load_sem.at[i]) for i, (name, (src, dst)) in enumerate(pairs.items())
    }
    late = ("qr", "qn", "ku", "vu", "wo")
    for name in loads:
        if name not in late:
            loads[name].start()

    nz = n_sp // 4
    z, side = me // 4, me % 4
    others = [lax.rem(side + i, 4) for i in range(1, 4)]
    levels = [lax.rem(z + i, nz) for i in range(1, nz)]
    greeted = [(z * 4 + s, mine) for s in others] + [(k * 4 + side, mine) for k in levels] + [(me, t) for t in partners]
    for other in greeted:
        pl.semaphore_signal(barrier, inc=1, device_id=other, device_id_type=MESH)

    feat, columns = shift_v.shape
    blocks = columns // LANES
    if part.shape[0] != MODS * blocks:
        part[...] = jnp.zeros_like(part)
    sides = []
    for name, ref in (("cond", cond_v), ("ctxm", ctxm_v)):
        loads[name].wait()
        value = ref[pl.ds(me, 1), :]
        value = value / (1.0 + jnp.exp(-value))
        sides.append(jnp.broadcast_to(value, (LANES, feat)).T)
    plan = ((shift_v, 0, "shift"), (shift_v, 1, None), (scale_v, 0, "scale"), (scale_v, 1, None), (gate_v, 0, "gate"))
    for row, (weight, which, name) in enumerate(plan):
        if name:
            loads[name].wait()
        for block in range(blocks):
            unit = row * blocks + block
            part[unit : unit + 1, :] = jnp.sum(
                weight[:, block * LANES : (block + 1) * LANES] * sides[which], axis=0, keepdims=True
            )
    for name in late:
        loads[name].start()
    pl.semaphore_wait(barrier, len(greeted))

    def spread(src, dst, at, sends, recvs, devices):
        copies = [
            remote(src, dst.at[at], sends.at[i], recvs.at[at], device) for i, device in enumerate(devices)
        ]
        for copy in copies:
            copy.start()
        return copies

    def fold(dst, recvs, indices):
        for i in indices:
            remote(dst.at[i], dst.at[i], send1.at[0], recvs.at[i], greeted[0]).wait_recv()
        total = dst[0]
        for i in range(1, dst.shape[0]):
            total = total + dst[i]
        return total

    sends = spread(part, land1, side, send1, recv1, [(z * 4 + s, mine) for s in others])
    land1[side] = part[...]
    loads["x"].wait()
    swaps = [remote(x_v.at[mine], x_v.at[mine], send_x.at[t], recv_x.at[mine], (me, t)) for t in partners]
    for swap in swaps:
        swap.start()

    loads["gain"].wait()
    loads["ctx"].wait()
    gain = gain_v[...]

    def norm(values):
        values = values.astype(F32)
        return values * lax.rsqrt(jnp.mean(values * values, axis=-1, keepdims=True) + EPS) * gain

    ctx = slot_of.ctx
    normed[:rows] = norm(x_v[mine])
    padded = ctx_v[...]
    if ctx != ctx_rows:
        padded = jnp.concatenate([padded.astype(F32), jnp.zeros((ctx - ctx_rows, depth), F32)], axis=0)
    normed[rows:] = norm(padded)

    loads["rowtab"].wait()
    loads["coltab"].wait()
    for k in range(tokens // GRID_W):
        line = pl.ds(me * (tokens // GRID_W) + k, 1)
        at = slice(k * GRID_W, (k + 1) * GRID_W)
        cos_v[at] = coltab_v[0] + rowtab_v[0, line]
        sin_v[at] = coltab_v[1] + rowtab_v[1, line]

    sum1[...] = fold(land1, recv1, others)
    sends += spread(sum1, land2, z, send2, recv2, [(k * 4 + side, mine) for k in levels])
    land2[z] = sum1[...]

    loads["vu"].wait()
    for at in range(0, vu_v.shape[1], LANES):
        vut[at : at + LANES, :] = vu_v[:, at : at + LANES].T
    loads["bias"].wait()
    for head in range(heads):
        bias_b[head] = jnp.broadcast_to(bias_v[:, head : head + 1] * LOG2E, bias_b.shape[1:])
    acc[...] = jnp.zeros_like(acc)
    top[...] = jnp.full(top.shape, -1e30, F32)
    total_v[...] = jnp.zeros_like(total_v)
    sum2[...] = fold(land2, recv2, levels)
    sends += spread(sum2, land3, mine, send3, recv3, [(me, t) for t in partners])
    land3[mine] = sum2[...]
    loads["down"].wait()
    loads["rope"].wait()
    loads["kvg"].wait()
    for t in partners:
        remote(land3.at[t], land3.at[t], send1.at[0], recv3.at[t], greeted[0]).wait_recv()
    for unit in range(MODS * blocks):
        row, block = unit // blocks, unit % blocks
        for t in range(n_tp):
            at = t * columns + block * LANES
            mods[row : row + 1, at : at + LANES] = land3[t, unit : unit + 1, :]

    def modulate(values, which):
        return (values * (1.0 + mods[2 + which : 3 + which, :]) + mods[which : which + 1, :]).astype(BF16)

    hown[:rows] = modulate(normed[:rows], 0)
    hown[rows:] = modulate(normed[rows:], 1)
    h = hown[...]
    inner = dot(h, down_v[...])
    inner = inner * lax.rsqrt(jnp.mean(inner * inner, axis=-1, keepdims=True) + EPS)
    inner = (inner * kvg_v[...]).astype(BF16)
    key = dot_nt(h, rope_v[...])
    key = jnp.concatenate([key, jnp.zeros((key.shape[0], LANES - rope), F32)], axis=1)
    own_rows = pl.ds(pl.multiple_of(mine * rows, rows), rows)
    turned = rotate(key[:rows], cos_v[own_rows], sin_v[own_rows])

    y, x = side // 2, side % 2
    odd = mine % 2
    flip_x = y * 2 + (1 - x)
    flip_y = (1 - y) * 2 + x
    side_a = flip_x * (1 - odd) + flip_y * odd
    side_b = flip_y * (1 - odd) + flip_x * odd
    side_ab = 3 - side

    own = (mine, z, side)
    for c in range(slot_of.columns):
        lanes = slice(c * LANES, (c + 1) * LANES)
        buf[mine, z, side, c * rows : (c + 1) * rows] = inner[:rows, lanes]
        at = slot_of.ctx_at + c * ctx
        buf[mine, z, side, at : at + ctx] = inner[rows:, lanes]
    shared = turned[: slot_of.rope_rows]
    if slot_of.split == 2:
        shared = shared + pltpu.roll(turned[slot_of.rope_rows :], rope, 1)
    buf[mine, z, side, slot_of.rope_at : slot_of.ctx_at] = shared.astype(BF16)
    buf[mine, z, side, slot_of.ctx_rope_at :] = key[rows:].astype(BF16)

    def plane(step, t):
        sign = 1 - 2 * (1 - t % 2)
        reach = jnp.minimum(z, nz - 1 - z)
        away = (step + 1) // 2
        near = z + (2 * (step % 2) - 1) * sign * away
        low = z <= nz - 1 - z
        far = lax.select(low, z * 0 + step, z * 0 + (nz - 1) - step)
        return lax.select(reach * 2 >= step, near, far)

    def slot(t, zz, ss):
        return buf.at[t, zz, ss]

    def peer(zz, ss):
        return (zz * 4 + ss, mine)

    def link(zz, ss, way, device):
        return remote(slot(mine, zz, ss), slot(mine, zz, ss), send.at[way, zz, ss], recv.at[zz, ss], device)

    def push(zz, ss, way, device, when=None):
        if when is None:
            link(zz, ss, way, device).start()
        else:
            pl.when(when)(lambda: link(zz, ss, way, device).start())

    def pushed(zz, ss, way, when=None):
        wait = lambda: link(zz, ss, way, peer(z, side_a)).wait_send()
        if when is None:
            wait()
        else:
            pl.when(when)(wait)

    def over(zz, ss, t):
        return remote(slot(mine, zz, ss), slot(mine, zz, ss), send_t.at[t, zz, ss], recv_t.at[mine, zz, ss], (me, t))

    def across(zz, ss):
        for t in partners:
            over(zz, ss, t).start()

    def arrived(zz, ss):
        link(zz, ss, 0, peer(z, side_a)).wait_recv()

    up, down = peer(lax.rem(z + 1, nz), side), peer(lax.rem(z + nz - 1, nz), side)
    to_a, to_b = peer(z, side_a), peer(z, side_b)

    def event_z(step):
        zz = plane(step, mine)
        if step == 0:
            push(zz, side, 3, to_b)
            push(zz, side, 2, to_a)
            push(zz, side, 0, up, z < nz - 1)
            push(zz, side, 1, down, z > 0)
        else:
            arrived(zz, side)
            push(zz, side, 0, up, (zz < z) & (z < nz - 1))
            push(zz, side, 1, down, (zz > z) & (z > 0))
            push(zz, side, 2, to_a)
            push(zz, side, 3, to_b)
        across(zz, side)

    def event_a(step):
        zz = plane(step, mine)
        arrived(zz, side_a)
        push(zz, side_a, 3, to_b)
        across(zz, side_a)

    def event_b(step, which):
        zz = plane(step, mine)
        arrived(zz, which)
        across(zz, which)

    def sent():
        for step in range(nz):
            zz = plane(step, mine)
            pushed(zz, side, 2)
            pushed(zz, side, 3)
            pushed(zz, side_a, 3)
            pushed(zz, side, 0, (zz <= z) & (z < nz - 1))
            pushed(zz, side, 1, (zz >= z) & (z > 0))
            for ss in (side, side_a, side_b, side_ab):
                for t in partners:
                    over(zz, ss, t).wait_send()

    event_z(0)

    hfull[mine] = hown[:rows]
    for t in partners:
        remote(x_v.at[t], x_v.at[t], send_x.at[t], recv_x.at[t], (me, t)).wait_recv()
        hfull[t] = modulate(norm(x_v[t]), 0)
    piece = hfull[...].reshape(tokens, depth)
    loads["qr"].wait()
    turned = dot(piece, qr_v[...])
    copies = turned.shape[1] // LANES
    turned = rotate(turned, jnp.concatenate([cos_v[...]] * copies, axis=1), jnp.concatenate([sin_v[...]] * copies, axis=1))
    turned = (turned * (factor * LOG2E)).T.astype(BF16)
    blank = jnp.zeros((LANES - rope, tokens), BF16)
    for head in range(heads):
        mine_rope = turned[head * rope : (head + 1) * rope]
        for g in range(slot_of.split):
            both = [mine_rope, blank] if g == 0 else [blank, mine_rope]
            qt[head, g, nope:, :] = jnp.concatenate(both, axis=0)
    loads["qn"].wait()
    wide = min(2 * nope, heads * nope)
    for at in range(0, heads * nope, wide):
        flatq = dot(piece, qn_v[:, at : at + wide]) * (factor * LOG2E)
        for k in range(wide // nope):
            value = flatq[:, k * nope : (k + 1) * nope].T.astype(BF16)
            for g in range(slot_of.split):
                qt[at // nope + k, g, :nope, :] = value
    loads["ku"].wait()

    def process(lat, ropes, biased=False, valid=None):
        count = lat.shape[0]
        tall = count // len(ropes)
        share = wide // nope

        def raise_keys(at):
            kbuf[:count, at : at + wide] = dot(lat, ku_v[:, at : at + wide]).astype(BF16)

        def raise_values(at):
            vt[at : at + wide, :count] = dot_nt(vut[at : at + wide, :], lat).astype(BF16)

        def score(head):
            if head % share == 0:
                raise_keys(head * nope)
            high = None
            for g, shared in enumerate(ropes):
                keys = jnp.concatenate(
                    [kbuf[g * tall : (g + 1) * tall, head * nope : (head + 1) * nope], shared], axis=1
                )
                piece = dot(keys, qt[head, g])
                if valid is not None:
                    piece = jnp.where(valid, piece, -1e30)
                sbuf[head % 2, g * tall : (g + 1) * tall] = piece
                peak = jnp.max(piece, axis=0, keepdims=True)
                high = peak if high is None else jnp.maximum(high, peak)
            return high

        def soften(head, high):
            old = top[head][:1]
            if biased:
                high = high + bias_b[head][:1]
            new = jnp.maximum(old, high)
            less = new - bias_b[head][:1] if biased else new
            weights = jnp.exp2(sbuf[head % 2, :count] - less)
            fade = jnp.exp2(old - new)
            top[head] = jnp.broadcast_to(new, top.shape[1:])
            total_v[head] = total_v[head] * fade + jnp.sum(weights, axis=0, keepdims=True)
            acc[head] = acc[head] * fade + dot(vt[head * nope : (head + 1) * nope, :count], weights.astype(BF16))

        high = score(0)
        raise_values(0)
        for head in range(heads):
            later = score(head + 1) if head + 1 < heads else None
            if head + 1 < heads and (head + 1) % share == 0:
                raise_values((head + 1) * nope)
            soften(head, high)
            high = later

    def chunk(k):
        step, half = k // 2, k % 2
        pair = (
            jnp.where(half == 0, side, flip_y),
            jnp.where(half == 0, flip_x, side_ab),
        )
        places = [(t, plane(step, t), ss) for t in range(n_tp) for ss in pair]
        for t in partners:
            zz = plane(step, t)
            for ss in pair:
                remote(slot(t, zz, ss), slot(t, zz, ss), send_t.at[t, zz, ss], recv_t.at[t, zz, ss], (me, t)).wait_recv()
        tall = slot_of.rope_rows

        def block(place, c, g):
            t, zz, ss = place
            return buf[t, zz, ss, c * rows + g * tall : c * rows + (g + 1) * tall]

        lat = jnp.concatenate(
            [
                jnp.concatenate([block(place, c, g) for g in range(slot_of.split) for place in places], axis=0)
                for c in range(slot_of.columns)
            ],
            axis=1,
        )
        ropes = jnp.concatenate(
            [buf[t, zz, ss, slot_of.rope_at : slot_of.ctx_at] for t, zz, ss in places], axis=0
        )
        process(lat, [ropes] * slot_of.split)

    kinds = {"z": event_z, "a": event_a, "b": lambda p: event_b(p, side_b), "d": lambda p: event_b(p, side_ab)}
    agenda = ORDERS.get(nz)
    if agenda is None:
        agenda = [
            [f"a{k}"] * (k < nz) + [f"z{k + 1}"] * (k + 1 < nz) + [f"{'bd'[k % 2]}{k // 2}"] for k in range(2 * nz)
        ]

    def before(k):
        for name in agenda[k]:
            kinds[name[0]](int(name[1:]))

    def turn(k, _):
        for i in range(2 * nz):
            pl.when(k == i)(functools.partial(before, i))
        chunk(k)
        return 0

    lax.fori_loop(0, 2 * nz, turn, 0)

    per_plane = slot_of.planes(n_tp, nz)

    def context_chunk(i, _):
        places = [
            (t, i * per_plane + dz, ss) for t in range(n_tp) for dz in range(per_plane) for ss in range(4)
        ]
        lat = jnp.concatenate(
            [
                jnp.concatenate(
                    [
                        buf[t, zz, ss, slot_of.ctx_at + c * ctx : slot_of.ctx_at + (c + 1) * ctx]
                        for t, zz, ss in places
                    ],
                    axis=0,
                )
                for c in range(slot_of.columns)
            ],
            axis=1,
        )
        ropes = jnp.concatenate([buf[t, zz, ss, slot_of.ctx_rope_at :] for t, zz, ss in places], axis=0)
        valid = None
        if ctx != ctx_rows:
            valid = lax.broadcasted_iota(jnp.int32, (lat.shape[0], tokens), 0) % ctx < ctx_rows
        process(lat, [ropes], True, valid)
        return 0

    if nz // per_plane == 1:
        context_chunk(0, 0)
    else:
        lax.fori_loop(0, nz // per_plane, context_chunk, 0)

    for head in range(heads):
        att[:, head * nope : (head + 1) * nope] = (acc[head] / total_v[head][:1]).T.astype(BF16)
    loads["wo"].wait()
    shipped = []
    for t in partners:
        lines = pl.ds(pl.multiple_of(t * rows, rows), rows)
        outbox[t] = dot(att[lines, :], wo_v[...]).astype(BF16)
        copy = remote(outbox.at[t], inbox.at[mine], send_o.at[t], recv_o.at[mine], (me, t))
        copy.start()
        shipped.append(copy)
    branch = dot(att[own_rows, :], wo_v[...]).astype(BF16).astype(F32)
    for t in partners:
        remote(outbox.at[t], inbox.at[t], send_o.at[t], recv_o.at[t], (me, t)).wait_recv()
        branch = branch + inbox[t].astype(F32)
    out_ref[...] = (x_v[mine].astype(F32) + mods[4:5, :] * branch).astype(BF16)
    for copy in sends + swaps + shipped:
        copy.wait_send()
    sent()


def tables(count, rope):
    quarter = rope // 4
    lane = np.arange(LANES)
    pair = (lane % rope) // 2
    inverse = (np.float32(ROPE_BASE) ** (-(pair % quarter).astype(np.float32) / np.float32(quarter))).astype(np.float32)
    is_row = (pair < quarter)[None, :]
    out = []
    for size, keep in ((count, is_row), (GRID_W, ~is_row)):
        angle = (np.arange(size, dtype=np.float32)[:, None] * inverse[None, :]).astype(np.float32)
        sine = np.sin(angle)
        signed = np.where(lane[None, :] % 2 == 0, -sine, sine)
        out.append(np.stack([np.where(keep, np.cos(angle), 0.0), np.where(keep, signed, 0.0)]).astype(np.float32))
    return out


def body(
    latent, cond, ctx_mod, context, shift_w, scale_w, gate_w, norm_gain, w_qn, w_qr, w_kv_down, w_rope_key,
    kv_gain, w_key_up, w_value_up, ctx_bias, w_out,
):
    n_sp, n_tp = lax.axis_size("sp"), lax.axis_size("tp")
    rows, width = latent.shape
    ctx_rows = context.shape[0]
    tokens = rows * n_tp
    heads = ctx_bias.shape[0]
    nope = w_key_up.shape[1] // heads
    rope = w_rope_key.shape[1]
    rank = w_kv_down.shape[1]
    factor = (nope + rope) ** (-0.5)
    feat, columns = shift_w.shape
    slot_of = Slot(rows, ctx_rows, rank)
    nz = n_sp // 4
    units = -(-MODS * (columns // LANES) // 8) * 8
    short = -(heads * rope) % LANES
    if short:
        w_qr = jnp.concatenate([w_qr, jnp.zeros((width, short), BF16)], axis=1)
    rowtab, coltab = tables(tokens * n_sp // GRID_W, rope)
    chunk_rows = n_tp * max(2 * rows, 4 * slot_of.ctx * slot_of.planes(n_tp, nz))

    def like(a):
        return pltpu.VMEM(a.shape, a.dtype)

    operands = (
        cond.reshape(n_sp, feat), ctx_mod.reshape(n_sp, feat), shift_w, scale_w, gate_w, latent, context,
        norm_gain[None, :], w_kv_down, w_rope_key.T, kv_gain[None, :], rowtab, coltab, ctx_bias[None, :],
        w_qr, w_qn, w_key_up, w_value_up, w_out,
    )
    staged = [like(a) for a in operands]
    staged[5] = pltpu.VMEM((n_tp, rows, width), BF16)
    dma = pltpu.SemaphoreType.DMA
    return pl.pallas_call(
        functools.partial(kernel, n_sp, n_tp, heads, nope, rope, ctx_rows, factor, slot_of),
        out_shape=jax.ShapeDtypeStruct((rows, width), BF16),
        in_specs=[pl.BlockSpec(memory_space=pl.ANY)] * len(operands),
        out_specs=pl.BlockSpec(memory_space=pltpu.VMEM),
        scratch_shapes=staged + [
            dma((len(operands),)),
            pltpu.VMEM((units, LANES), F32),
            pltpu.VMEM((4, units, LANES), F32),
            pltpu.VMEM((units, LANES), F32),
            pltpu.VMEM((nz, units, LANES), F32),
            pltpu.VMEM((units, LANES), F32),
            pltpu.VMEM((n_tp, units, LANES), F32),
            pltpu.VMEM((8, width), F32),
            pltpu.VMEM((rows + slot_of.ctx, width), F32),
            pltpu.VMEM((rows + slot_of.ctx, width), BF16),
            pltpu.VMEM((n_tp, rows, width), BF16),
            pltpu.VMEM((tokens, LANES), F32),
            pltpu.VMEM((tokens, LANES), F32),
            pltpu.VMEM((w_value_up.shape[1], rank), BF16),
            pltpu.VMEM((heads, 8, tokens), F32),
            pltpu.VMEM((n_tp, nz, 4, slot_of.height, LANES), BF16),
            pltpu.VMEM((heads, slot_of.split, nope + LANES, tokens), BF16),
            pltpu.VMEM((chunk_rows, heads * nope), BF16),
            pltpu.VMEM((heads * nope, chunk_rows), BF16),
            pltpu.VMEM((2, chunk_rows, tokens), F32),
            pltpu.VMEM((heads, nope, tokens), F32),
            pltpu.VMEM((heads, 8, tokens), F32),
            pltpu.VMEM((heads, 8, tokens), F32),
            pltpu.VMEM((tokens, heads * nope), BF16),
            pltpu.VMEM((n_tp, rows, width), BF16),
            pltpu.VMEM((n_tp, rows, width), BF16),
            dma((4,)),
            dma((4,)),
            dma((nz,)),
            dma((nz,)),
            dma((n_tp,)),
            dma((n_tp,)),
            dma((n_tp,)),
            dma((n_tp,)),
            dma((4, nz, 4)),
            dma((nz, 4)),
            dma((n_tp, nz, 4)),
            dma((n_tp, nz, 4)),
            dma((n_tp,)),
            dma((n_tp,)),
        ],
        compiler_params=pltpu.CompilerParams(
            collective_id=0, has_side_effects=True, vmem_limit_bytes=62 * 1024 * 1024
        ),
        name="block",
    )(*operands)


def solution(mesh):
    placed = (
        P(("sp", "tp"), None),
        P(),
        P(),
        P(("sp", "tp"), None),
        P("sp", "tp"),
        P("sp", "tp"),
        P("sp", "tp"),
        P(),
        P(None, "tp"),
        P(None, "tp"),
        P(),
        P(),
        P(),
        P(None, "tp"),
        P(None, "tp"),
        P("tp"),
        P("tp", None),
    )
    return jax.shard_map(
        body, mesh=mesh, in_specs=placed, out_specs=P(("sp", "tp"), None), check_vma=False
    )
```

```python
import functools

import jax
import jax.numpy as jnp
import numpy as np
from jax import lax
from jax.experimental import pallas as pl
from jax.experimental.pallas import tpu as pltpu
from jax.sharding import PartitionSpec as P

GRID_W = 128
EPS = 1e-06
ROPE_BASE = 10000.0
LANES = 128
LOG2E = 1.4426950408889634
MODS = 5
ORDERS = {
    4: (
        ("a0", "z1", "b0", "z2"), ("d0", "a1"), ("a2", "b1", "z3", "d1"), ("b2", "d2"), ("a3",), ("b3",), ("d3",), (),
    )
}
MESH = pl.DeviceIdType.MESH
F32 = jnp.float32
BF16 = jnp.bfloat16


def remote(src, dst, send, recv, device):
    return pltpu.make_async_remote_copy(
        src_ref=src, dst_ref=dst, send_sem=send, recv_sem=recv, device_id=device, device_id_type=MESH
    )


def rotate(values, cosine, sine):
    width = values.shape[-1]
    ahead = pltpu.roll(values, width - 1, 1)
    behind = pltpu.roll(values, 1, 1)
    even = lax.broadcasted_iota(jnp.int32, values.shape, 1) % 2 == 0
    return values * cosine + jnp.where(even, ahead, behind) * sine


def dot(a, b):
    return jnp.dot(a, b, preferred_element_type=F32)


def dot_nt(a, b):
    return lax.dot_general(a, b, (((1,), (1,)), ((), ())), preferred_element_type=F32)


class Slot:
    def __init__(self, rows, ctx_rows, rank):
        self.split = 2 if rows % 32 == 0 else 1
        self.rows = rows
        self.ctx = -(-ctx_rows // 16) * 16
        self.columns = rank // LANES
        self.stride = rows + self.ctx
        self.rope_at = self.columns * self.stride
        self.rope_rows = rows // self.split
        self.ctx_rope_at = self.rope_at + self.rope_rows
        self.height = self.ctx_rope_at + self.ctx

    def planes(self, n_tp, nz):
        return max(1, min(nz, 512 // (self.ctx * 4 * n_tp)))


def kernel(
    n_sp, n_tp, heads, nope, rope, ctx_rows, factor, slot_of,
    cond_hbm, ctxm_hbm, shift_hbm, scale_hbm, gate_hbm, latent_hbm, context_hbm, gain_hbm, down_hbm, rope_hbm,
    kvg_hbm, rowtab_hbm, coltab_hbm, bias_hbm, qr_hbm, qn_hbm, ku_hbm, vu_hbm, wo_hbm,
    out_ref,
    cond_v, ctxm_v, shift_v, scale_v, gate_v, x_v, ctx_v, gain_v, down_v, rope_v, kvg_v, rowtab_v, coltab_v, bias_v,
    qr_v, qn_v, ku_v, vu_v, wo_v, load_sem,
    part, land1, sum1, land2, sum2, land3, mods, normed, hown, hfull, cos_v, sin_v, vut, kut, bias_b,
    buf, qt, dense, kbuf, vt, sbuf, acc, top, total_v, att, outbox, inbox,
    send1, recv1, send2, recv2, send3, recv3, send_x, recv_x, send, recv, send_t, recv_t, send_o, recv_o,
):
    me = lax.axis_index("sp")
    mine = lax.axis_index("tp")
    barrier = pltpu.get_barrier_semaphore()
    rows, rank = slot_of.rows, ku_v.shape[0]
    depth = x_v.shape[2]
    tokens = n_tp * rows
    partners = [lax.rem(mine + i, n_tp) for i in range(1, n_tp)]

    pairs = dict(
        cond=(cond_hbm, cond_v), ctxm=(ctxm_hbm, ctxm_v), shift=(shift_hbm, shift_v), scale=(scale_hbm, scale_v),
        gate=(gate_hbm, gate_v), x=(latent_hbm, x_v.at[mine]), ctx=(context_hbm, ctx_v), gain=(gain_hbm, gain_v),
        down=(down_hbm, down_v), rope=(rope_hbm, rope_v), kvg=(kvg_hbm, kvg_v), rowtab=(rowtab_hbm, rowtab_v),
        coltab=(coltab_hbm, coltab_v), bias=(bias_hbm, bias_v), qr=(qr_hbm, qr_v), qn=(qn_hbm, qn_v),
        ku=(ku_hbm, ku_v), vu=(vu_hbm, vu_v), wo=(wo_hbm, wo_v),
    )
    loads = {
        name: pltpu.make_async_copy(src, dst, load_sem.at[i]) for i, (name, (src, dst)) in enumerate(pairs.items())
    }
    late = ("qr", "qn", "ku", "vu", "wo")
    for name in loads:
        if name not in late:
            loads[name].start()

    nz = n_sp // 4
    z, side = me // 4, me % 4
    others = [lax.rem(side + i, 4) for i in range(1, 4)]
    levels = [lax.rem(z + i, nz) for i in range(1, nz)]
    greeted = [(z * 4 + s, mine) for s in others] + [(k * 4 + side, mine) for k in levels] + [(me, t) for t in partners]
    for other in greeted:
        pl.semaphore_signal(barrier, inc=1, device_id=other, device_id_type=MESH)

    feat, columns = shift_v.shape
    blocks = columns // LANES
    if part.shape[0] != MODS * blocks:
        part[...] = jnp.zeros_like(part)
    sides = []
    for name, ref in (("cond", cond_v), ("ctxm", ctxm_v)):
        loads[name].wait()
        value = ref[pl.ds(me, 1), :]
        value = value / (1.0 + jnp.exp(-value))
        sides.append(jnp.broadcast_to(value, (LANES, feat)).T)
    plan = ((shift_v, 0, "shift"), (shift_v, 1, None), (scale_v, 0, "scale"), (scale_v, 1, None), (gate_v, 0, "gate"))
    for row, (weight, which, name) in enumerate(plan):
        if name:
            loads[name].wait()
        for block in range(blocks):
            unit = row * blocks + block
            part[unit : unit + 1, :] = jnp.sum(
                weight[:, block * LANES : (block + 1) * LANES] * sides[which], axis=0, keepdims=True
            )
    for name in late:
        loads[name].start()
    pl.semaphore_wait(barrier, len(greeted))

    def spread(src, dst, at, sends, recvs, devices):
        copies = [
            remote(src, dst.at[at], sends.at[i], recvs.at[at], device) for i, device in enumerate(devices)
        ]
        for copy in copies:
            copy.start()
        return copies

    def fold(dst, recvs, indices):
        for i in indices:
            remote(dst.at[i], dst.at[i], send1.at[0], recvs.at[i], greeted[0]).wait_recv()
        total = dst[0]
        for i in range(1, dst.shape[0]):
            total = total + dst[i]
        return total

    sends = spread(part, land1, side, send1, recv1, [(z * 4 + s, mine) for s in others])
    land1[side] = part[...]
    loads["x"].wait()
    swaps = [remote(x_v.at[mine], x_v.at[mine], send_x.at[t], recv_x.at[mine], (me, t)) for t in partners]
    for swap in swaps:
        swap.start()

    loads["gain"].wait()
    loads["ctx"].wait()
    gain = gain_v[...]

    def norm(values):
        values = values.astype(F32)
        return values * lax.rsqrt(jnp.mean(values * values, axis=-1, keepdims=True) + EPS) * gain

    ctx = slot_of.ctx
    normed[:rows] = norm(x_v[mine])
    padded = ctx_v[...]
    if ctx != ctx_rows:
        padded = jnp.concatenate([padded.astype(F32), jnp.zeros((ctx - ctx_rows, depth), F32)], axis=0)
    normed[rows:] = norm(padded)

    loads["rowtab"].wait()
    loads["coltab"].wait()
    for k in range(tokens // GRID_W):
        line = pl.ds(me * (tokens // GRID_W) + k, 1)
        at = slice(k * GRID_W, (k + 1) * GRID_W)
        cos_v[at] = coltab_v[0] + rowtab_v[0, line]
        sin_v[at] = coltab_v[1] + rowtab_v[1, line]

    sum1[...] = fold(land1, recv1, others)
    sends += spread(sum1, land2, z, send2, recv2, [(k * 4 + side, mine) for k in levels])
    land2[z] = sum1[...]

    loads["vu"].wait()
    for at in range(0, vu_v.shape[1], LANES):
        vut[at : at + LANES, :] = vu_v[:, at : at + LANES].T
    loads["bias"].wait()
    for head in range(heads):
        bias_b[head] = jnp.broadcast_to(bias_v[:, head : head + 1] * LOG2E, bias_b.shape[1:])
    acc[...] = jnp.zeros_like(acc)
    top[...] = jnp.full(top.shape, -1e30, F32)
    total_v[...] = jnp.zeros_like(total_v)
    sum2[...] = fold(land2, recv2, levels)
    sends += spread(sum2, land3, mine, send3, recv3, [(me, t) for t in partners])
    land3[mine] = sum2[...]
    loads["down"].wait()
    loads["rope"].wait()
    loads["kvg"].wait()
    for t in partners:
        remote(land3.at[t], land3.at[t], send1.at[0], recv3.at[t], greeted[0]).wait_recv()
    for unit in range(MODS * blocks):
        row, block = unit // blocks, unit % blocks
        for t in range(n_tp):
            at = t * columns + block * LANES
            mods[row : row + 1, at : at + LANES] = land3[t, unit : unit + 1, :]

    def modulate(values, which):
        return (values * (1.0 + mods[2 + which : 3 + which, :]) + mods[which : which + 1, :]).astype(BF16)

    hown[:rows] = modulate(normed[:rows], 0)
    hown[rows:] = modulate(normed[rows:], 1)
    h = hown[...]
    inner = dot(h, down_v[...])
    inner = inner * lax.rsqrt(jnp.mean(inner * inner, axis=-1, keepdims=True) + EPS)
    inner = (inner * kvg_v[...]).astype(BF16)
    key = dot_nt(h, rope_v[...])
    key = jnp.concatenate([key, jnp.zeros((key.shape[0], LANES - rope), F32)], axis=1)
    own_rows = pl.ds(pl.multiple_of(mine * rows, rows), rows)
    turned = rotate(key[:rows], cos_v[own_rows], sin_v[own_rows])

    y, x = side // 2, side % 2
    odd = mine % 2
    flip_x = y * 2 + (1 - x)
    flip_y = (1 - y) * 2 + x
    side_a = flip_x * (1 - odd) + flip_y * odd
    side_b = flip_y * (1 - odd) + flip_x * odd
    side_ab = 3 - side

    own = (mine, z, side)
    for c in range(slot_of.columns):
        lanes = slice(c * LANES, (c + 1) * LANES)
        buf[mine, z, side, c * slot_of.stride : c * slot_of.stride + rows] = inner[:rows, lanes]
        at = c * slot_of.stride + rows
        buf[mine, z, side, at : at + ctx] = inner[rows:, lanes]
    shared = turned[: slot_of.rope_rows]
    if slot_of.split == 2:
        shared = shared + pltpu.roll(turned[slot_of.rope_rows :], rope, 1)
    buf[mine, z, side, slot_of.rope_at : slot_of.ctx_rope_at] = shared.astype(BF16)
    buf[mine, z, side, slot_of.ctx_rope_at :] = key[rows:].astype(BF16)

    def plane(step, t):
        sign = 1 - 2 * (1 - t % 2)
        reach = jnp.minimum(z, nz - 1 - z)
        away = (step + 1) // 2
        near = z + (2 * (step % 2) - 1) * sign * away
        low = z <= nz - 1 - z
        far = lax.select(low, z * 0 + step, z * 0 + (nz - 1) - step)
        return lax.select(reach * 2 >= step, near, far)

    def slot(t, zz, ss):
        return buf.at[t, zz, ss]

    def peer(zz, ss):
        return (zz * 4 + ss, mine)

    def link(zz, ss, way, device):
        return remote(slot(mine, zz, ss), slot(mine, zz, ss), send.at[way, zz, ss], recv.at[zz, ss], device)

    def push(zz, ss, way, device, when=None):
        if when is None:
            link(zz, ss, way, device).start()
        else:
            pl.when(when)(lambda: link(zz, ss, way, device).start())

    def pushed(zz, ss, way, when=None):
        wait = lambda: link(zz, ss, way, peer(z, side_a)).wait_send()
        if when is None:
            wait()
        else:
            pl.when(when)(wait)

    def over(zz, ss, t):
        return remote(slot(mine, zz, ss), slot(mine, zz, ss), send_t.at[t, zz, ss], recv_t.at[mine, zz, ss], (me, t))

    def across(zz, ss):
        for t in partners:
            over(zz, ss, t).start()

    def arrived(zz, ss):
        link(zz, ss, 0, peer(z, side_a)).wait_recv()

    up, down = peer(lax.rem(z + 1, nz), side), peer(lax.rem(z + nz - 1, nz), side)
    to_a, to_b = peer(z, side_a), peer(z, side_b)

    def event_z(step):
        zz = plane(step, mine)
        if step == 0:
            push(zz, side, 3, to_b)
            push(zz, side, 2, to_a)
            push(zz, side, 0, up, z < nz - 1)
            push(zz, side, 1, down, z > 0)
        else:
            arrived(zz, side)
            push(zz, side, 0, up, (zz < z) & (z < nz - 1))
            push(zz, side, 1, down, (zz > z) & (z > 0))
            push(zz, side, 2, to_a)
            push(zz, side, 3, to_b)
        across(zz, side)

    def event_a(step):
        zz = plane(step, mine)
        arrived(zz, side_a)
        push(zz, side_a, 3, to_b)
        across(zz, side_a)

    def event_b(step, which):
        zz = plane(step, mine)
        arrived(zz, which)
        across(zz, which)

    def sent():
        for step in range(nz):
            zz = plane(step, mine)
            pushed(zz, side, 2)
            pushed(zz, side, 3)
            pushed(zz, side_a, 3)
            pushed(zz, side, 0, (zz <= z) & (z < nz - 1))
            pushed(zz, side, 1, (zz >= z) & (z > 0))
            for ss in (side, side_a, side_b, side_ab):
                for t in partners:
                    over(zz, ss, t).wait_send()

    event_z(0)

    hfull[mine] = hown[:rows]
    for t in partners:
        remote(x_v.at[t], x_v.at[t], send_x.at[t], recv_x.at[t], (me, t)).wait_recv()
        hfull[t] = modulate(norm(x_v[t]), 0)
    piece = hfull[...].reshape(tokens, depth)
    loads["qr"].wait()
    turned = dot(piece, qr_v[...])
    copies = turned.shape[1] // LANES
    turned = rotate(turned, jnp.concatenate([cos_v[...]] * copies, axis=1), jnp.concatenate([sin_v[...]] * copies, axis=1))
    turned = (turned * (factor * LOG2E)).T.astype(BF16)
    blank = jnp.zeros((LANES - rope, tokens), BF16)
    for head in range(heads):
        mine_rope = turned[head * rope : (head + 1) * rope]
        for g in range(slot_of.split):
            both = [mine_rope, blank] if g == 0 else [blank, mine_rope]
            qt[head, g, nope:, :] = jnp.concatenate(both, axis=0)
    loads["qn"].wait()
    wide = min(2 * nope, heads * nope)
    for at in range(0, heads * nope, wide):
        flatq = dot(piece, qn_v[:, at : at + wide]) * (factor * LOG2E)
        for k in range(wide // nope):
            value = flatq[:, k * nope : (k + 1) * nope].T.astype(BF16)
            for g in range(slot_of.split):
                qt[at // nope + k, g, :nope, :] = value
    loads["ku"].wait()
    for at in range(0, ku_v.shape[1], LANES):
        kut[at : at + LANES, :] = ku_v[:, at : at + LANES].T

    def process(lat, ropes, biased=False, valid=None):
        count = lat.shape[0]
        dense[:count] = lat
        tall = count // len(ropes)
        share = wide // nope

        def raise_keys(at):
            kbuf[:count, at : at + wide] = dot_nt(dense[:count], kut[at : at + wide, :]).astype(BF16)

        def raise_values(at):
            vt[at : at + wide, :count] = dot_nt(vut[at : at + wide, :], dense[:count]).astype(BF16)

        def score(head):
            if head % share == 0:
                raise_keys(head * nope)
            high = None
            for g, shared in enumerate(ropes):
                keys = jnp.concatenate(
                    [kbuf[g * tall : (g + 1) * tall, head * nope : (head + 1) * nope], shared], axis=1
                )
                piece = dot(keys, qt[head, g])
                if valid is not None:
                    piece = jnp.where(valid, piece, -1e30)
                sbuf[head % 2, g * tall : (g + 1) * tall] = piece
                peak = jnp.max(piece, axis=0, keepdims=True)
                high = peak if high is None else jnp.maximum(high, peak)
            return high

        def soften(head, high):
            old = top[head][:1]
            if biased:
                high = high + bias_b[head][:1]
            new = jnp.maximum(old, high)
            less = new - bias_b[head][:1] if biased else new
            weights = jnp.exp2(sbuf[head % 2, :count] - less)
            fade = jnp.exp2(old - new)
            top[head] = jnp.broadcast_to(new, top.shape[1:])
            total_v[head] = total_v[head] * fade + jnp.sum(weights, axis=0, keepdims=True)
            acc[head] = acc[head] * fade + dot(vt[head * nope : (head + 1) * nope, :count], weights.astype(BF16))

        high = score(0)
        for head in range(heads):
            later = score(head + 1) if head + 1 < heads else None
            if head % share == 0:
                raise_values(head * nope)
            soften(head, high)
            high = later

    def chunk(entries):
        places = [(t, plane(step, t), ss) for t in range(n_tp) for step, ss in entries]
        for t in partners:
            for step, ss in entries:
                zz = plane(step, t)
                remote(slot(t, zz, ss), slot(t, zz, ss), send_t.at[t, zz, ss], recv_t.at[t, zz, ss], (me, t)).wait_recv()
        tall = slot_of.rope_rows

        def block(place, c, g):
            t, zz, ss = place
            at = c * slot_of.stride + g * tall
            return buf[t, zz, ss, at : at + tall]

        lat = jnp.concatenate(
            [
                jnp.concatenate([block(place, c, g) for g in range(slot_of.split) for place in places], axis=0)
                for c in range(slot_of.columns)
            ],
            axis=1,
        )
        ropes = jnp.concatenate(
            [buf[t, zz, ss, slot_of.rope_at : slot_of.ctx_rope_at] for t, zz, ss in places], axis=0
        )
        process(lat, [ropes] * slot_of.split)

    kinds = {"z": event_z, "a": event_a, "b": lambda p: event_b(p, side_b), "d": lambda p: event_b(p, side_ab)}
    agenda = ORDERS.get(nz)
    if agenda is None:
        agenda = [
            [f"a{k}"] * (k < nz) + [f"z{k + 1}"] * (k + 1 < nz) + [f"{'bd'[k % 2]}{k // 2}"] for k in range(2 * nz)
        ]

    def before(k):
        for name in agenda[k]:
            kinds[name[0]](int(name[1:]))

    def turn(k, _):
        for i in range(2 * nz - 1):
            pl.when(k == i)(functools.partial(before, i))
        step, late = k // 2, k % 2
        chunk(
            [
                (step, flip_x * (1 - late) + side_ab * late),
                (step + late, flip_y * (1 - late) + side * late),
            ]
        )
        return 0

    chunk([(0, side)])
    lax.fori_loop(0, 2 * nz - 1, turn, 0)
    before(2 * nz - 1)
    chunk([(nz - 1, side_ab)])

    per_plane = slot_of.planes(n_tp, nz)

    def context_chunk(i, _):
        places = [
            (t, i * per_plane + dz, ss) for t in range(n_tp) for dz in range(per_plane) for ss in range(4)
        ]
        lat = jnp.concatenate(
            [
                jnp.concatenate(
                    [
                        buf[t, zz, ss, c * slot_of.stride + rows : (c + 1) * slot_of.stride]
                        for t, zz, ss in places
                    ],
                    axis=0,
                )
                for c in range(slot_of.columns)
            ],
            axis=1,
        )
        ropes = jnp.concatenate([buf[t, zz, ss, slot_of.ctx_rope_at :] for t, zz, ss in places], axis=0)
        valid = None
        if ctx != ctx_rows:
            valid = lax.broadcasted_iota(jnp.int32, (lat.shape[0], tokens), 0) % ctx < ctx_rows
        process(lat, [ropes], True, valid)
        return 0

    if nz // per_plane == 1:
        context_chunk(0, 0)
    else:
        lax.fori_loop(0, nz // per_plane, context_chunk, 0)

    for head in range(heads):
        att[:, head * nope : (head + 1) * nope] = (acc[head] / total_v[head][:1]).T.astype(BF16)
    loads["wo"].wait()
    shipped = []
    for t in partners:
        lines = pl.ds(pl.multiple_of(t * rows, rows), rows)
        outbox[t] = dot(att[lines, :], wo_v[...]).astype(BF16)
        copy = remote(outbox.at[t], inbox.at[mine], send_o.at[t], recv_o.at[mine], (me, t))
        copy.start()
        shipped.append(copy)
    branch = dot(att[own_rows, :], wo_v[...]).astype(BF16).astype(F32)
    for t in partners:
        remote(outbox.at[t], inbox.at[t], send_o.at[t], recv_o.at[t], (me, t)).wait_recv()
        branch = branch + inbox[t].astype(F32)
    out_ref[...] = (x_v[mine].astype(F32) + mods[4:5, :] * branch).astype(BF16)
    for copy in sends + swaps + shipped:
        copy.wait_send()
    sent()


def tables(count, rope):
    quarter = rope // 4
    lane = np.arange(LANES)
    pair = (lane % rope) // 2
    inverse = (np.float32(ROPE_BASE) ** (-(pair % quarter).astype(np.float32) / np.float32(quarter))).astype(np.float32)
    is_row = (pair < quarter)[None, :]
    out = []
    for size, keep in ((count, is_row), (GRID_W, ~is_row)):
        angle = (np.arange(size, dtype=np.float32)[:, None] * inverse[None, :]).astype(np.float32)
        sine = np.sin(angle)
        signed = np.where(lane[None, :] % 2 == 0, -sine, sine)
        out.append(np.stack([np.where(keep, np.cos(angle), 0.0), np.where(keep, signed, 0.0)]).astype(np.float32))
    return out


def body(
    latent, cond, ctx_mod, context, shift_w, scale_w, gate_w, norm_gain, w_qn, w_qr, w_kv_down, w_rope_key,
    kv_gain, w_key_up, w_value_up, ctx_bias, w_out,
):
    n_sp, n_tp = lax.axis_size("sp"), lax.axis_size("tp")
    rows, width = latent.shape
    ctx_rows = context.shape[0]
    tokens = rows * n_tp
    heads = ctx_bias.shape[0]
    nope = w_key_up.shape[1] // heads
    rope = w_rope_key.shape[1]
    rank = w_kv_down.shape[1]
    factor = (nope + rope) ** (-0.5)
    feat, columns = shift_w.shape
    slot_of = Slot(rows, ctx_rows, rank)
    nz = n_sp // 4
    units = -(-MODS * (columns // LANES) // 8) * 8
    short = -(heads * rope) % LANES
    if short:
        w_qr = jnp.concatenate([w_qr, jnp.zeros((width, short), BF16)], axis=1)
    rowtab, coltab = tables(tokens * n_sp // GRID_W, rope)
    chunk_rows = n_tp * max(2 * rows, 4 * slot_of.ctx * slot_of.planes(n_tp, nz))

    def like(a):
        return pltpu.VMEM(a.shape, a.dtype)

    operands = (
        cond.reshape(n_sp, feat), ctx_mod.reshape(n_sp, feat), shift_w, scale_w, gate_w, latent, context,
        norm_gain[None, :], w_kv_down, w_rope_key.T, kv_gain[None, :], rowtab, coltab, ctx_bias[None, :],
        w_qr, w_qn, w_key_up, w_value_up, w_out,
    )
    staged = [like(a) for a in operands]
    staged[5] = pltpu.VMEM((n_tp, rows, width), BF16)
    dma = pltpu.SemaphoreType.DMA
    return pl.pallas_call(
        functools.partial(kernel, n_sp, n_tp, heads, nope, rope, ctx_rows, factor, slot_of),
        out_shape=jax.ShapeDtypeStruct((rows, width), BF16),
        in_specs=[pl.BlockSpec(memory_space=pl.ANY)] * len(operands),
        out_specs=pl.BlockSpec(memory_space=pltpu.VMEM),
        scratch_shapes=staged + [
            dma((len(operands),)),
            pltpu.VMEM((units, LANES), F32),
            pltpu.VMEM((4, units, LANES), F32),
            pltpu.VMEM((units, LANES), F32),
            pltpu.VMEM((nz, units, LANES), F32),
            pltpu.VMEM((units, LANES), F32),
            pltpu.VMEM((n_tp, units, LANES), F32),
            pltpu.VMEM((8, width), F32),
            pltpu.VMEM((rows + slot_of.ctx, width), F32),
            pltpu.VMEM((rows + slot_of.ctx, width), BF16),
            pltpu.VMEM((n_tp, rows, width), BF16),
            pltpu.VMEM((tokens, LANES), F32),
            pltpu.VMEM((tokens, LANES), F32),
            pltpu.VMEM((w_value_up.shape[1], rank), BF16),
            pltpu.VMEM((w_key_up.shape[1], rank), BF16),
            pltpu.VMEM((heads, 8, tokens), F32),
            pltpu.VMEM((n_tp, nz, 4, slot_of.height, LANES), BF16),
            pltpu.VMEM((heads, slot_of.split, nope + LANES, tokens), BF16),
            pltpu.VMEM((chunk_rows, rank), BF16),
            pltpu.VMEM((chunk_rows, heads * nope), BF16),
            pltpu.VMEM((heads * nope, chunk_rows), BF16),
            pltpu.VMEM((2, chunk_rows, tokens), F32),
            pltpu.VMEM((heads, nope, tokens), F32),
            pltpu.VMEM((heads, 8, tokens), F32),
            pltpu.VMEM((heads, 8, tokens), F32),
            pltpu.VMEM((tokens, heads * nope), BF16),
            pltpu.VMEM((n_tp, rows, width), BF16),
            pltpu.VMEM((n_tp, rows, width), BF16),
            dma((4,)),
            dma((4,)),
            dma((nz,)),
            dma((nz,)),
            dma((n_tp,)),
            dma((n_tp,)),
            dma((n_tp,)),
            dma((n_tp,)),
            dma((4, nz, 4)),
            dma((nz, 4)),
            dma((n_tp, nz, 4)),
            dma((n_tp, nz, 4)),
            dma((n_tp,)),
            dma((n_tp,)),
        ],
        compiler_params=pltpu.CompilerParams(
            collective_id=0, has_side_effects=True, vmem_limit_bytes=62 * 1024 * 1024
        ),
        name="block",
    )(*operands)


def solution(mesh):
    placed = (
        P(("sp", "tp"), None),
        P(),
        P(),
        P(("sp", "tp"), None),
        P("sp", "tp"),
        P("sp", "tp"),
        P("sp", "tp"),
        P(),
        P(None, "tp"),
        P(None, "tp"),
        P(),
        P(),
        P(),
        P(None, "tp"),
        P(None, "tp"),
        P("tp"),
        P("tp", None),
    )
    return jax.shard_map(
        body, mesh=mesh, in_specs=placed, out_specs=P(("sp", "tp"), None), check_vma=False
    )
```

```python
import functools

import jax
import jax.numpy as jnp
import numpy as np
from jax import lax
from jax.experimental import pallas as pl
from jax.experimental.pallas import tpu as pltpu
from jax.sharding import PartitionSpec as P

GRID_W = 128
EPS = 1e-06
ROPE_BASE = 10000.0
LANES = 128
LOG2E = 1.4426950408889634
MODS = 5
ORDERS = {
    4: (
        ("a0", "z1", "b0", "z2"), ("d0", "a1"), ("a2", "b1", "z3", "d1"), ("b2", "d2"), ("a3",), ("b3",), ("d3",), (),
    )
}
MESH = pl.DeviceIdType.MESH
F32 = jnp.float32
BF16 = jnp.bfloat16


def remote(src, dst, send, recv, device):
    return pltpu.make_async_remote_copy(
        src_ref=src, dst_ref=dst, send_sem=send, recv_sem=recv, device_id=device, device_id_type=MESH
    )


def rotate(values, cosine, sine):
    width = values.shape[-1]
    ahead = pltpu.roll(values, width - 1, 1)
    behind = pltpu.roll(values, 1, 1)
    even = lax.broadcasted_iota(jnp.int32, values.shape, 1) % 2 == 0
    return values * cosine + jnp.where(even, ahead, behind) * sine


def dot(a, b):
    return jnp.dot(a, b, preferred_element_type=F32)


def dot_nt(a, b):
    return lax.dot_general(a, b, (((1,), (1,)), ((), ())), preferred_element_type=F32)


class Slot:
    def __init__(self, rows, ctx_rows, rank):
        self.split = 2 if rows % 32 == 0 else 1
        self.rows = rows
        self.ctx = -(-ctx_rows // 16) * 16
        self.columns = rank // LANES
        self.stride = rows + self.ctx
        self.rope_at = self.columns * self.stride
        self.rope_rows = rows // self.split
        self.ctx_rope_at = self.rope_at + self.rope_rows
        self.height = self.ctx_rope_at + self.ctx

    def planes(self, n_tp, nz):
        return max(1, min(nz, 512 // (self.ctx * 4 * n_tp)))


def kernel(
    n_sp, n_tp, heads, nope, rope, ctx_rows, factor, slot_of,
    cond_hbm, ctxm_hbm, shift_hbm, scale_hbm, gate_hbm, latent_hbm, context_hbm, gain_hbm, down_hbm, rope_hbm,
    kvg_hbm, rowtab_hbm, coltab_hbm, bias_hbm, qr_hbm, qn_hbm, ku_hbm, vu_hbm, wo_hbm,
    out_ref,
    cond_v, ctxm_v, shift_v, scale_v, gate_v, x_v, ctx_v, gain_v, down_v, rope_v, kvg_v, rowtab_v, coltab_v, bias_v,
    qr_v, qn_v, ku_v, vu_v, wo_v, load_sem,
    part, land1, sum1, land2, sum2, land3, mods, normed, hown, hfull, cos_v, sin_v, vut, kut, bias_b,
    buf, qt, dense, kbuf, vt, sbuf, acc, top, total_v, att, outbox, inbox,
    send1, recv1, send2, recv2, send3, recv3, send_x, recv_x, send, recv, send_t, recv_t, send_o, recv_o,
):
    me = lax.axis_index("sp")
    mine = lax.axis_index("tp")
    barrier = pltpu.get_barrier_semaphore()
    rows, rank = slot_of.rows, ku_v.shape[0]
    depth = x_v.shape[2]
    tokens = n_tp * rows
    partners = [lax.rem(mine + i, n_tp) for i in range(1, n_tp)]

    pairs = dict(
        cond=(cond_hbm, cond_v), ctxm=(ctxm_hbm, ctxm_v), shift=(shift_hbm, shift_v), scale=(scale_hbm, scale_v),
        gate=(gate_hbm, gate_v), x=(latent_hbm, x_v.at[mine]), ctx=(context_hbm, ctx_v), gain=(gain_hbm, gain_v),
        down=(down_hbm, down_v), rope=(rope_hbm, rope_v), kvg=(kvg_hbm, kvg_v), rowtab=(rowtab_hbm, rowtab_v),
        coltab=(coltab_hbm, coltab_v), bias=(bias_hbm, bias_v), qr=(qr_hbm, qr_v), qn=(qn_hbm, qn_v),
        ku=(ku_hbm, ku_v), vu=(vu_hbm, vu_v), wo=(wo_hbm, wo_v),
    )
    loads = {
        name: pltpu.make_async_copy(src, dst, load_sem.at[i]) for i, (name, (src, dst)) in enumerate(pairs.items())
    }
    late = ("qr", "qn", "ku", "vu", "wo")
    for name in loads:
        if name not in late:
            loads[name].start()

    nz = n_sp // 4
    z, side = me // 4, me % 4
    others = [lax.rem(side + i, 4) for i in range(1, 4)]
    levels = [lax.rem(z + i, nz) for i in range(1, nz)]
    greeted = [(z * 4 + s, mine) for s in others] + [(k * 4 + side, mine) for k in levels] + [(me, t) for t in partners]
    for other in greeted:
        pl.semaphore_signal(barrier, inc=1, device_id=other, device_id_type=MESH)

    feat, columns = shift_v.shape
    blocks = columns // LANES
    if part.shape[0] != MODS * blocks:
        part[...] = jnp.zeros_like(part)
    sides = []
    for name, ref in (("cond", cond_v), ("ctxm", ctxm_v)):
        loads[name].wait()
        value = ref[pl.ds(me, 1), :]
        value = value / (1.0 + jnp.exp(-value))
        sides.append(jnp.broadcast_to(value, (LANES, feat)).T)
    plan = ((shift_v, 0, "shift"), (shift_v, 1, None), (scale_v, 0, "scale"), (scale_v, 1, None), (gate_v, 0, "gate"))
    for row, (weight, which, name) in enumerate(plan):
        if name:
            loads[name].wait()
        for block in range(blocks):
            unit = row * blocks + block
            part[unit : unit + 1, :] = jnp.sum(
                weight[:, block * LANES : (block + 1) * LANES] * sides[which], axis=0, keepdims=True
            )
    for name in late:
        loads[name].start()
    pl.semaphore_wait(barrier, len(greeted))

    def spread(src, dst, at, sends, recvs, devices):
        copies = [
            remote(src, dst.at[at], sends.at[i], recvs.at[at], device) for i, device in enumerate(devices)
        ]
        for copy in copies:
            copy.start()
        return copies

    def fold(dst, recvs, indices):
        for i in indices:
            remote(dst.at[i], dst.at[i], send1.at[0], recvs.at[i], greeted[0]).wait_recv()
        total = dst[0]
        for i in range(1, dst.shape[0]):
            total = total + dst[i]
        return total

    sends = spread(part, land1, side, send1, recv1, [(z * 4 + s, mine) for s in others])
    land1[side] = part[...]
    loads["x"].wait()
    swaps = [remote(x_v.at[mine], x_v.at[mine], send_x.at[t], recv_x.at[mine], (me, t)) for t in partners]
    for swap in swaps:
        swap.start()

    loads["gain"].wait()
    loads["ctx"].wait()
    gain = gain_v[...]

    def norm(values):
        values = values.astype(F32)
        return values * lax.rsqrt(jnp.mean(values * values, axis=-1, keepdims=True) + EPS) * gain

    ctx = slot_of.ctx
    normed[:rows] = norm(x_v[mine])
    padded = ctx_v[...]
    if ctx != ctx_rows:
        padded = jnp.concatenate([padded.astype(F32), jnp.zeros((ctx - ctx_rows, depth), F32)], axis=0)
    normed[rows:] = norm(padded)

    loads["rowtab"].wait()
    loads["coltab"].wait()
    for k in range(tokens // GRID_W):
        line = pl.ds(me * (tokens // GRID_W) + k, 1)
        at = slice(k * GRID_W, (k + 1) * GRID_W)
        cos_v[at] = coltab_v[0] + rowtab_v[0, line]
        sin_v[at] = coltab_v[1] + rowtab_v[1, line]

    sum1[...] = fold(land1, recv1, others)
    sends += spread(sum1, land2, z, send2, recv2, [(k * 4 + side, mine) for k in levels])
    land2[z] = sum1[...]

    loads["vu"].wait()
    for at in range(0, vu_v.shape[1], LANES):
        vut[at : at + LANES, :] = vu_v[:, at : at + LANES].T
    loads["bias"].wait()
    for head in range(heads):
        bias_b[head] = jnp.broadcast_to(bias_v[:, head : head + 1] * LOG2E, bias_b.shape[1:])
    acc[...] = jnp.zeros_like(acc)
    top[...] = jnp.full(top.shape, -1e30, F32)
    total_v[...] = jnp.zeros_like(total_v)
    sum2[...] = fold(land2, recv2, levels)
    sends += spread(sum2, land3, mine, send3, recv3, [(me, t) for t in partners])
    land3[mine] = sum2[...]
    loads["down"].wait()
    loads["rope"].wait()
    loads["kvg"].wait()
    for t in partners:
        remote(land3.at[t], land3.at[t], send1.at[0], recv3.at[t], greeted[0]).wait_recv()
    for unit in range(MODS * blocks):
        row, block = unit // blocks, unit % blocks
        for t in range(n_tp):
            at = t * columns + block * LANES
            mods[row : row + 1, at : at + LANES] = land3[t, unit : unit + 1, :]

    def modulate(values, which):
        return (values * (1.0 + mods[2 + which : 3 + which, :]) + mods[which : which + 1, :]).astype(BF16)

    hown[:rows] = modulate(normed[:rows], 0)
    hown[rows:] = modulate(normed[rows:], 1)
    h = hown[...]
    inner = dot(h, down_v[...])
    inner = inner * lax.rsqrt(jnp.mean(inner * inner, axis=-1, keepdims=True) + EPS)
    inner = (inner * kvg_v[...]).astype(BF16)
    key = dot_nt(h, rope_v[...])
    key = jnp.concatenate([key, jnp.zeros((key.shape[0], LANES - rope), F32)], axis=1)
    own_rows = pl.ds(pl.multiple_of(mine * rows, rows), rows)
    turned = rotate(key[:rows], cos_v[own_rows], sin_v[own_rows])

    y, x = side // 2, side % 2
    odd = mine % 2
    flip_x = y * 2 + (1 - x)
    flip_y = (1 - y) * 2 + x
    side_a = flip_x * (1 - odd) + flip_y * odd
    side_b = flip_y * (1 - odd) + flip_x * odd
    side_ab = 3 - side

    own = (mine, z, side)
    for c in range(slot_of.columns):
        lanes = slice(c * LANES, (c + 1) * LANES)
        buf[mine, z, side, c * slot_of.stride : c * slot_of.stride + rows] = inner[:rows, lanes]
        at = c * slot_of.stride + rows
        buf[mine, z, side, at : at + ctx] = inner[rows:, lanes]
    shared = turned[: slot_of.rope_rows]
    if slot_of.split == 2:
        shared = shared + pltpu.roll(turned[slot_of.rope_rows :], rope, 1)
    buf[mine, z, side, slot_of.rope_at : slot_of.ctx_rope_at] = shared.astype(BF16)
    buf[mine, z, side, slot_of.ctx_rope_at :] = key[rows:].astype(BF16)

    def plane(step, t):
        sign = 1 - 2 * (1 - t % 2)
        reach = jnp.minimum(z, nz - 1 - z)
        away = (step + 1) // 2
        near = z + (2 * (step % 2) - 1) * sign * away
        low = z <= nz - 1 - z
        far = lax.select(low, z * 0 + step, z * 0 + (nz - 1) - step)
        return lax.select(reach * 2 >= step, near, far)

    def slot(t, zz, ss):
        return buf.at[t, zz, ss]

    def peer(zz, ss):
        return (zz * 4 + ss, mine)

    def link(zz, ss, way, device):
        return remote(slot(mine, zz, ss), slot(mine, zz, ss), send.at[way, zz, ss], recv.at[zz, ss], device)

    def push(zz, ss, way, device, when=None):
        if when is None:
            link(zz, ss, way, device).start()
        else:
            pl.when(when)(lambda: link(zz, ss, way, device).start())

    def pushed(zz, ss, way, when=None):
        wait = lambda: link(zz, ss, way, peer(z, side_a)).wait_send()
        if when is None:
            wait()
        else:
            pl.when(when)(wait)

    def over(zz, ss, t):
        return remote(slot(mine, zz, ss), slot(mine, zz, ss), send_t.at[t, zz, ss], recv_t.at[mine, zz, ss], (me, t))

    def across(zz, ss):
        for t in partners:
            over(zz, ss, t).start()

    def arrived(zz, ss):
        link(zz, ss, 0, peer(z, side_a)).wait_recv()

    up, down = peer(lax.rem(z + 1, nz), side), peer(lax.rem(z + nz - 1, nz), side)
    to_a, to_b = peer(z, side_a), peer(z, side_b)

    def event_z(step):
        zz = plane(step, mine)
        if step == 0:
            push(zz, side, 3, to_b)
            push(zz, side, 2, to_a)
            push(zz, side, 0, up, z < nz - 1)
            push(zz, side, 1, down, z > 0)
        else:
            arrived(zz, side)
            push(zz, side, 0, up, (zz < z) & (z < nz - 1))
            push(zz, side, 1, down, (zz > z) & (z > 0))
            push(zz, side, 2, to_a)
            push(zz, side, 3, to_b)
        across(zz, side)

    def event_a(step):
        zz = plane(step, mine)
        arrived(zz, side_a)
        push(zz, side_a, 3, to_b)
        across(zz, side_a)

    def event_b(step, which):
        zz = plane(step, mine)
        arrived(zz, which)
        across(zz, which)

    def sent():
        for step in range(nz):
            zz = plane(step, mine)
            pushed(zz, side, 2)
            pushed(zz, side, 3)
            pushed(zz, side_a, 3)
            pushed(zz, side, 0, (zz <= z) & (z < nz - 1))
            pushed(zz, side, 1, (zz >= z) & (z > 0))
            for ss in (side, side_a, side_b, side_ab):
                for t in partners:
                    over(zz, ss, t).wait_send()

    event_z(0)

    hfull[mine] = hown[:rows]
    for t in partners:
        remote(x_v.at[t], x_v.at[t], send_x.at[t], recv_x.at[t], (me, t)).wait_recv()
        hfull[t] = modulate(norm(x_v[t]), 0)
    piece = hfull[...].reshape(tokens, depth)
    loads["qr"].wait()
    turned = dot(piece, qr_v[...])
    copies = turned.shape[1] // LANES
    turned = rotate(turned, jnp.concatenate([cos_v[...]] * copies, axis=1), jnp.concatenate([sin_v[...]] * copies, axis=1))
    turned = (turned * (factor * LOG2E)).T.astype(BF16)
    blank = jnp.zeros((LANES - rope, tokens), BF16)
    for head in range(heads):
        mine_rope = turned[head * rope : (head + 1) * rope]
        for g in range(slot_of.split):
            both = [mine_rope, blank] if g == 0 else [blank, mine_rope]
            qt[head, g, nope:, :] = jnp.concatenate(both, axis=0)
    loads["qn"].wait()
    wide = min(2 * nope, heads * nope)
    for at in range(0, heads * nope, wide):
        flatq = dot(piece, qn_v[:, at : at + wide]) * (factor * LOG2E)
        for k in range(wide // nope):
            value = flatq[:, k * nope : (k + 1) * nope].T.astype(BF16)
            for g in range(slot_of.split):
                qt[at // nope + k, g, :nope, :] = value
    loads["ku"].wait()
    for at in range(0, ku_v.shape[1], LANES):
        kut[at : at + LANES, :] = ku_v[:, at : at + LANES].T

    def process(lat, ropes, biased=False, valid=None):
        count = lat.shape[0]
        dense[:count] = lat
        tall = count // len(ropes)
        share = wide // nope

        def raise_keys(at):
            kbuf[:count, at : at + wide] = dot_nt(dense[:count], kut[at : at + wide, :]).astype(BF16)

        def raise_values(at):
            vt[at : at + wide, :count] = dot_nt(vut[at : at + wide, :], dense[:count]).astype(BF16)

        def score(head):
            if head % share == 0:
                raise_keys(head * nope)
            high = None
            for g, shared in enumerate(ropes):
                keys = jnp.concatenate(
                    [kbuf[g * tall : (g + 1) * tall, head * nope : (head + 1) * nope], shared], axis=1
                )
                piece = dot(keys, qt[head, g])
                if valid is not None:
                    piece = jnp.where(valid, piece, -1e30)
                sbuf[head % 2, g * tall : (g + 1) * tall] = piece
                peak = jnp.max(piece, axis=0, keepdims=True)
                high = peak if high is None else jnp.maximum(high, peak)
            return high

        def soften(head, high):
            old = top[head][:1]
            if biased:
                high = high + bias_b[head][:1]
            new = jnp.maximum(old, high)
            less = new - bias_b[head][:1] if biased else new
            weights = jnp.exp2(sbuf[head % 2, :count] - less)
            fade = jnp.exp2(old - new)
            top[head] = jnp.broadcast_to(new, top.shape[1:])
            total_v[head] = total_v[head] * fade + jnp.sum(weights, axis=0, keepdims=True)
            acc[head] = acc[head] * fade + dot(vt[head * nope : (head + 1) * nope, :count], weights.astype(BF16))

        high = score(0)
        for head in range(heads):
            later = score(head + 1) if head + 1 < heads else None
            if head % share == 0:
                raise_values(head * nope)
            soften(head, high)
            high = later

    def chunk(entries):
        places = [(t, plane(step, t), ss) for t in range(n_tp) for step, ss in entries]
        for t in partners:
            for step, ss in entries:
                zz = plane(step, t)
                remote(slot(t, zz, ss), slot(t, zz, ss), send_t.at[t, zz, ss], recv_t.at[t, zz, ss], (me, t)).wait_recv()
        tall = slot_of.rope_rows

        def block(place, c, g):
            t, zz, ss = place
            at = c * slot_of.stride + g * tall
            return buf[t, zz, ss, at : at + tall]

        lat = jnp.concatenate(
            [
                jnp.concatenate([block(place, c, g) for g in range(slot_of.split) for place in places], axis=0)
                for c in range(slot_of.columns)
            ],
            axis=1,
        )
        ropes = jnp.concatenate(
            [buf[t, zz, ss, slot_of.rope_at : slot_of.ctx_rope_at] for t, zz, ss in places], axis=0
        )
        process(lat, [ropes] * slot_of.split)

    kinds = {"z": event_z, "a": event_a, "b": lambda p: event_b(p, side_b), "d": lambda p: event_b(p, side_ab)}
    agenda = ORDERS.get(nz)
    if agenda is None:
        agenda = [
            [f"a{k}"] * (k < nz) + [f"z{k + 1}"] * (k + 1 < nz) + [f"{'bd'[k % 2]}{k // 2}"] for k in range(2 * nz)
        ]

    def before(k):
        for name in agenda[k]:
            kinds[name[0]](int(name[1:]))

    def turn(k, _):
        for i in range(2 * nz - 1):
            pl.when(k == i)(functools.partial(before, i))
        step, late = k // 2, k % 2
        chunk(
            [
                (step, flip_x * (1 - late) + side_ab * late),
                (step + late, flip_y * (1 - late) + side * late),
            ]
        )
        return 0

    chunk([(0, side)])
    lax.fori_loop(0, 2 * nz - 1, turn, 0)
    before(2 * nz - 1)
    chunk([(nz - 1, side_ab)])

    per_plane = slot_of.planes(n_tp, nz)

    def context_chunk(i, _):
        places = [
            (t, i * per_plane + dz, ss) for t in range(n_tp) for dz in range(per_plane) for ss in range(4)
        ]
        lat = jnp.concatenate(
            [
                jnp.concatenate(
                    [
                        buf[t, zz, ss, c * slot_of.stride + rows : (c + 1) * slot_of.stride]
                        for t, zz, ss in places
                    ],
                    axis=0,
                )
                for c in range(slot_of.columns)
            ],
            axis=1,
        )
        ropes = jnp.concatenate([buf[t, zz, ss, slot_of.ctx_rope_at :] for t, zz, ss in places], axis=0)
        valid = None
        if ctx != ctx_rows:
            valid = lax.broadcasted_iota(jnp.int32, (lat.shape[0], tokens), 0) % ctx < ctx_rows
        process(lat, [ropes], True, valid)
        return 0

    if nz // per_plane == 1:
        context_chunk(0, 0)
    else:
        lax.fori_loop(0, nz // per_plane, context_chunk, 0)

    for head in range(heads):
        att[:, head * nope : (head + 1) * nope] = (acc[head] / total_v[head][:1]).T.astype(BF16)
    loads["wo"].wait()
    shipped = []
    for t in partners:
        lines = pl.ds(pl.multiple_of(t * rows, rows), rows)
        for part_of in range(2):
            cut = slice(part_of * depth // 2, (part_of + 1) * depth // 2)
            outbox[part_of, t] = dot(att[lines, :], wo_v[:, cut]).astype(BF16)
            copy = remote(
                outbox.at[part_of, t], inbox.at[part_of, mine], send_o.at[part_of, t], recv_o.at[part_of, mine], (me, t)
            )
            copy.start()
            shipped.append(copy)
    branch = dot(att[own_rows, :], wo_v[...]).astype(BF16).astype(F32)
    for part_of in range(2):
        cut = slice(part_of * depth // 2, (part_of + 1) * depth // 2)
        piece = branch[:, cut]
        for t in partners:
            remote(
                outbox.at[part_of, t], inbox.at[part_of, t], send_o.at[part_of, t], recv_o.at[part_of, t], (me, t)
            ).wait_recv()
            piece = piece + inbox[part_of, t].astype(F32)
        out_ref[:, cut] = (x_v[mine, :, cut].astype(F32) + mods[4:5, cut] * piece).astype(BF16)
    for copy in sends + swaps + shipped:
        copy.wait_send()
    sent()


def tables(count, rope):
    quarter = rope // 4
    lane = np.arange(LANES)
    pair = (lane % rope) // 2
    inverse = (np.float32(ROPE_BASE) ** (-(pair % quarter).astype(np.float32) / np.float32(quarter))).astype(np.float32)
    is_row = (pair < quarter)[None, :]
    out = []
    for size, keep in ((count, is_row), (GRID_W, ~is_row)):
        angle = (np.arange(size, dtype=np.float32)[:, None] * inverse[None, :]).astype(np.float32)
        sine = np.sin(angle)
        signed = np.where(lane[None, :] % 2 == 0, -sine, sine)
        out.append(np.stack([np.where(keep, np.cos(angle), 0.0), np.where(keep, signed, 0.0)]).astype(np.float32))
    return out


def body(
    latent, cond, ctx_mod, context, shift_w, scale_w, gate_w, norm_gain, w_qn, w_qr, w_kv_down, w_rope_key,
    kv_gain, w_key_up, w_value_up, ctx_bias, w_out,
):
    n_sp, n_tp = lax.axis_size("sp"), lax.axis_size("tp")
    rows, width = latent.shape
    ctx_rows = context.shape[0]
    tokens = rows * n_tp
    heads = ctx_bias.shape[0]
    nope = w_key_up.shape[1] // heads
    rope = w_rope_key.shape[1]
    rank = w_kv_down.shape[1]
    factor = (nope + rope) ** (-0.5)
    feat, columns = shift_w.shape
    slot_of = Slot(rows, ctx_rows, rank)
    nz = n_sp // 4
    units = -(-MODS * (columns // LANES) // 8) * 8
    short = -(heads * rope) % LANES
    if short:
        w_qr = jnp.concatenate([w_qr, jnp.zeros((width, short), BF16)], axis=1)
    rowtab, coltab = tables(tokens * n_sp // GRID_W, rope)
    chunk_rows = n_tp * max(2 * rows, 4 * slot_of.ctx * slot_of.planes(n_tp, nz))

    def like(a):
        return pltpu.VMEM(a.shape, a.dtype)

    operands = (
        cond.reshape(n_sp, feat), ctx_mod.reshape(n_sp, feat), shift_w, scale_w, gate_w, latent, context,
        norm_gain[None, :], w_kv_down, w_rope_key.T, kv_gain[None, :], rowtab, coltab, ctx_bias[None, :],
        w_qr, w_qn, w_key_up, w_value_up, w_out,
    )
    staged = [like(a) for a in operands]
    staged[5] = pltpu.VMEM((n_tp, rows, width), BF16)
    dma = pltpu.SemaphoreType.DMA
    return pl.pallas_call(
        functools.partial(kernel, n_sp, n_tp, heads, nope, rope, ctx_rows, factor, slot_of),
        out_shape=jax.ShapeDtypeStruct((rows, width), BF16),
        in_specs=[pl.BlockSpec(memory_space=pl.ANY)] * len(operands),
        out_specs=pl.BlockSpec(memory_space=pltpu.VMEM),
        scratch_shapes=staged + [
            dma((len(operands),)),
            pltpu.VMEM((units, LANES), F32),
            pltpu.VMEM((4, units, LANES), F32),
            pltpu.VMEM((units, LANES), F32),
            pltpu.VMEM((nz, units, LANES), F32),
            pltpu.VMEM((units, LANES), F32),
            pltpu.VMEM((n_tp, units, LANES), F32),
            pltpu.VMEM((8, width), F32),
            pltpu.VMEM((rows + slot_of.ctx, width), F32),
            pltpu.VMEM((rows + slot_of.ctx, width), BF16),
            pltpu.VMEM((n_tp, rows, width), BF16),
            pltpu.VMEM((tokens, LANES), F32),
            pltpu.VMEM((tokens, LANES), F32),
            pltpu.VMEM((w_value_up.shape[1], rank), BF16),
            pltpu.VMEM((w_key_up.shape[1], rank), BF16),
            pltpu.VMEM((heads, 8, tokens), F32),
            pltpu.VMEM((n_tp, nz, 4, slot_of.height, LANES), BF16),
            pltpu.VMEM((heads, slot_of.split, nope + LANES, tokens), BF16),
            pltpu.VMEM((chunk_rows, rank), BF16),
            pltpu.VMEM((chunk_rows, heads * nope), BF16),
            pltpu.VMEM((heads * nope, chunk_rows), BF16),
            pltpu.VMEM((2, chunk_rows, tokens), F32),
            pltpu.VMEM((heads, nope, tokens), F32),
            pltpu.VMEM((heads, 8, tokens), F32),
            pltpu.VMEM((heads, 8, tokens), F32),
            pltpu.VMEM((tokens, heads * nope), BF16),
            pltpu.VMEM((2, n_tp, rows, width // 2), BF16),
            pltpu.VMEM((2, n_tp, rows, width // 2), BF16),
            dma((4,)),
            dma((4,)),
            dma((nz,)),
            dma((nz,)),
            dma((n_tp,)),
            dma((n_tp,)),
            dma((n_tp,)),
            dma((n_tp,)),
            dma((4, nz, 4)),
            dma((nz, 4)),
            dma((n_tp, nz, 4)),
            dma((n_tp, nz, 4)),
            dma((2, n_tp)),
            dma((2, n_tp)),
        ],
        compiler_params=pltpu.CompilerParams(
            collective_id=0, has_side_effects=True, vmem_limit_bytes=62 * 1024 * 1024
        ),
        name="block",
    )(*operands)


def solution(mesh):
    placed = (
        P(("sp", "tp"), None),
        P(),
        P(),
        P(("sp", "tp"), None),
        P("sp", "tp"),
        P("sp", "tp"),
        P("sp", "tp"),
        P(),
        P(None, "tp"),
        P(None, "tp"),
        P(),
        P(),
        P(),
        P(None, "tp"),
        P(None, "tp"),
        P("tp"),
        P("tp", None),
    )
    return jax.shard_map(
        body, mesh=mesh, in_specs=placed, out_specs=P(("sp", "tp"), None), check_vma=False
    )
```
